256 devices in a mesh: grp: 2 (over y), sp: 16 (over z), tp: 8 (over x, core).
Axes of the slice: x: 4, y: 2, z: 16, core: 2. Of those that a mesh axis runs over, the one named last changes fastest.
The devices are a block of a 4x16x16 slice.
Arguments:
- tokens_in: bfloat16 [12288, 4096], P(('grp', 'sp')), parts along dimension 0, may hold values from -6 to 6
- norm_gain: float32 [4096], replicated, may hold values from 0.1 to 1.9
- window_query: bfloat16 [4096, 1024], P('sp', 'tp'), may hold values from -0.09375 to 0.09375
- window_key: bfloat16 [4096, 512], P('sp', 'tp'), may hold values from -0.09375 to 0.09375
- window_value: bfloat16 [4096, 512], P('sp', 'tp'), may hold values from -0.09375 to 0.09375
- window_query_gain: float32 [64], replicated, may hold values from 0.6 to 16
- window_key_gain: float32 [64], replicated, may hold values from 0.6 to 16
- sink_logit: float32 [16], P('tp'), may hold values from 1 to 6
- dense_query: bfloat16 [4096, 1024], P('sp', 'tp'), may hold values from -0.09375 to 0.09375
- dense_key: bfloat16 [4096, 512], P('sp', 'tp'), may hold values from -0.09375 to 0.09375
- dense_value: bfloat16 [4096, 512], P('sp', 'tp'), may hold values from -0.09375 to 0.09375
- dense_query_gain: float32 [64], replicated, may hold values from 1 to 14
- dense_key_gain: float32 [64], replicated, may hold values from 1 to 14
- window_out: bfloat16 [1024, 4096], P('tp', 'sp'), may hold values from -1.5 to 1.5
- dense_out: bfloat16 [1024, 4096], P('tp', 'sp'), may hold values from -3 to 3
Outputs:
- mixed_out: bfloat16 [12288, 4096], P(('grp', 'sp', 'tp')), parts along dimension 0
The draws below stay inside these ranges and needn't reach their ends.
There are 2 independent parts, one for each index of `grp`. The reference program is written for one: setup_inputs(seed, part) draws one part's arguments, and reference() takes and returns one part's arrays. A program takes and returns all parts, laid end to end along the dimension named above; an argument that names none is the same for every part. Nothing has to cross between parts.
All inputs are finite; a program needn't handle non-finite values.
Results may differ from the reference program's by a relative error of at most 0.03.
The reference program's roundings to bfloat16 on the way count: a program that leaves them out, or rounds other values in their place, can miss the bound.
Values may be sent and summed in bfloat16 or wider, within the bound.
A program may use at most 64 MiB of HBM per device.

```python
import jax
import jax.numpy as jnp
from jax import lax

D = 4096
B_HEADS = 16
B_KV = 8
C_HEADS = 16
C_KV = 8
HD = 64
WINDOW = 128
GRID_W = 64
TOKENS = 6144
N_TP = 8


def gain_values(key, salt, low, high, hidden_low, hidden_high):
    subkey = jax.random.fold_in(key, salt)
    return jax.random.uniform(subkey, (HD,), jnp.float32, low, high)


def draw_window_query_gain(key, part):
    return gain_values(key, 101, 0.6, 1.6, 12.0, 16.0)


def draw_window_key_gain(key, part):
    return gain_values(key, 102, 0.6, 1.6, 12.0, 16.0)


def draw_dense_query_gain(key, part):
    return gain_values(key, 103, 1.0, 1.8, 10.0, 14.0)


def draw_dense_key_gain(key, part):
    return gain_values(key, 104, 1.0, 1.8, 10.0, 14.0)


def steps_of(key, shape, pieces, least, top_value):
    loudness = 1.0
    for axis_at, blocks in pieces:
        draws = jax.random.uniform(jax.random.fold_in(jax.random.fold_in(key, 6), axis_at), (blocks,), jnp.float32, least / len(pieces), top_value / len(pieces))
        loudness = loudness * jnp.repeat(jnp.exp(draws), shape[axis_at] // blocks).reshape((-1,) + (1,) * (len(shape) - 1 - axis_at))
    return loudness


def noise(key, extent, deviation, reach, cuts=(), held_as=jnp.bfloat16):
    loudness = steps_of(key, extent, cuts, -0.22, 0.18) if cuts else 1.0
    entries = jax.random.normal(key, extent, jnp.float32) * deviation * loudness
    return jnp.minimum(jnp.maximum(entries, -reach), reach).astype(held_as)


def setup_inputs(seed: int = 0, part: int = 0) -> dict:
    seeds = jax.random.split(jax.random.key(seed), 16)
    part_splits = jax.random.split(jax.random.fold_in(seeds[15], part), 16)
    tokens_in = noise(part_splits[0], (TOKENS, D), 1.0, 6.0, ((0, 16),))
    norm_gain = jnp.clip(1.0 + 0.18 * jax.random.normal(seeds[1], (D,), jnp.float32), 0.1, 1.9)
    window_query = noise(seeds[2], (D, B_HEADS * HD), D ** -0.5, 0.09375, ((0, 16), (1, 8)))
    window_key = noise(seeds[3], (D, B_KV * HD), D ** -0.5, 0.09375, ((0, 16), (1, 8)))
    window_value = noise(seeds[4], (D, B_KV * HD), D ** -0.5, 0.09375, ((0, 16), (1, 8)))
    window_query_gain = draw_window_query_gain(jax.random.fold_in(seeds[15], 71), part)
    window_key_gain = draw_window_key_gain(jax.random.fold_in(seeds[15], 71), part)
    sink_logit = jnp.clip(1.0 + 5.0 * jax.random.uniform(seeds[7], (B_HEADS,), jnp.float32) ** steps_of(seeds[7], (B_HEADS,), ((0, 8),), -0.2, 0.2), 1.0, 6.0)
    dense_query = noise(seeds[8], (D, C_HEADS * HD), D ** -0.5, 0.09375, ((0, 16), (1, 8)))
    dense_key = noise(seeds[9], (D, C_KV * HD), D ** -0.5, 0.09375, ((0, 16), (1, 8)))
    dense_value = noise(seeds[10], (D, C_KV * HD), D ** -0.5, 0.09375, ((0, 16), (1, 8)))
    dense_query_gain = draw_dense_query_gain(jax.random.fold_in(seeds[15], 71), part)
    dense_key_gain = draw_dense_key_gain(jax.random.fold_in(seeds[15], 71), part)
    window_out = noise(seeds[13], (B_HEADS * HD, D), 0.25, 1.5, ((0, 8), (1, 16)))
    dense_out = noise(seeds[14], (C_HEADS * HD, D), 0.5, 3.0, ((0, 8), (1, 16)))
    return {"tokens_in": tokens_in, "norm_gain": norm_gain, "window_query": window_query, "window_key": window_key, "window_value": window_value, "window_query_gain": window_query_gain, "window_key_gain": window_key_gain, "sink_logit": sink_logit, "dense_query": dense_query, "dense_key": dense_key, "dense_value": dense_value, "dense_query_gain": dense_query_gain, "dense_key_gain": dense_key_gain, "window_out": window_out, "dense_out": dense_out}


EPS = 1e-06
THETA = 10000.0

def store(values):
    return lax.optimization_barrier(values.astype(jnp.bfloat16))

def rope_table(places, width):
    inverse = THETA ** (-jnp.arange(0, width, 2, dtype=jnp.float32) / width)
    angles = places.astype(jnp.float32)[:, None] * inverse[None, :]
    angles = jnp.concatenate([angles, angles], axis=-1)
    return (jnp.cos(angles), jnp.sin(angles))

def turn(values, tables):
    cosine, sine = tables
    middle = values.shape[-1] // 2
    rotated = jnp.concatenate([-values[..., middle:], values[..., :middle]], axis=-1)
    return values * cosine[:, None, :] + rotated * sine[:, None, :]

def head_norm(projected, gain):
    width = gain.shape[0]
    heads = projected.reshape(projected.shape[0], -1, width)
    return heads * lax.rsqrt(lax.optimization_barrier(jnp.mean(heads * heads, axis=-1, keepdims=True)) + EPS) * gain

def line_heads(projected, gain, places):
    normed = head_norm(projected, gain)
    return turn(normed, rope_table(places, gain.shape[0])).reshape(projected.shape)

def grid_heads(projected, gain, places):
    normed = head_norm(projected, gain)
    middle = gain.shape[0] // 2
    by_row = turn(normed[..., :middle], rope_table(places // GRID_W, middle))
    by_col = turn(normed[..., middle:], rope_table(places % GRID_W, middle))
    return jnp.concatenate([by_row, by_col], axis=-1).reshape(projected.shape)

def banded(query, keys_ext, values_ext, offset, total_len, sink_logit):
    length = query.shape[0]
    kv_heads = keys_ext.shape[1] // HD
    group_size = query.shape[1] // (HD * kv_heads)
    block_count = length // WINDOW
    query_blocks = query.astype(jnp.float32).reshape(block_count, WINDOW, kv_heads, group_size, HD)
    key_blocks = keys_ext.astype(jnp.float32).reshape(block_count + 2, WINDOW, kv_heads, HD)
    value_blocks = values_ext.astype(jnp.float32).reshape(block_count + 2, WINDOW, kv_heads, HD)
    key_near = jnp.concatenate([key_blocks[:-2], key_blocks[1:-1], key_blocks[2:]], axis=1)
    value_near = jnp.concatenate([value_blocks[:-2], value_blocks[1:-1], value_blocks[2:]], axis=1)
    scores = jnp.einsum('nqhgd,nkhd->nhgqk', query_blocks, key_near) * HD ** (-0.5)
    query_pos = offset + jnp.arange(length, dtype=jnp.int32).reshape(block_count, WINDOW)
    key_pos = offset - WINDOW + (jnp.arange(block_count, dtype=jnp.int32)[:, None] * WINDOW + jnp.arange(3 * WINDOW, dtype=jnp.int32)[None, :])
    valid = (jnp.abs(query_pos[:, :, None] - key_pos[:, None, :]) <= WINDOW) & (key_pos >= 0)[:, None, :] & (key_pos < total_len)[:, None, :]
    scores = jnp.where(valid[:, None, None], scores, -jnp.inf)
    floor = sink_logit.reshape(kv_heads, group_size)[None, :, :, None, None]
    top = jnp.maximum(lax.optimization_barrier(jnp.max(scores, axis=-1, keepdims=True)), floor)
    expon = jnp.exp(scores - top)
    weights = store(expon / (lax.optimization_barrier(jnp.sum(expon, axis=-1, keepdims=True)) + jnp.exp(floor - top)))
    result = jnp.einsum('nhgqk,nkhd->nqhgd', weights.astype(jnp.float32), value_near)
    return result.reshape(length, -1)

def dense_attention(query, keys, values):
    length = query.shape[0]
    kv_heads = keys.shape[1] // HD
    group_size = query.shape[1] // (HD * kv_heads)
    if length % 256 == 0:
        block = 256
    elif length % 128 == 0:
        block = 128
    else:
        block = length
    query_blocks = query.astype(jnp.float32).reshape(length // block, block, kv_heads, group_size, HD)
    key_heads = keys.astype(jnp.float32).reshape(length, kv_heads, HD)
    value_heads = values.astype(jnp.float32).reshape(length, kv_heads, HD)

    def one_block(query_block):
        scores = jnp.einsum('qhgd,khd->hgqk', query_block, key_heads) * HD ** (-0.5)
        top = lax.optimization_barrier(jnp.max(scores, axis=-1, keepdims=True))
        expon = jnp.exp(scores - top)
        total = lax.optimization_barrier(jnp.sum(expon, axis=-1))
        rounded = store(expon).astype(jnp.float32)
        summed = jnp.einsum('hgqk,khd->qhgd', rounded, value_heads)
        return summed / jnp.transpose(total, (2, 0, 1))[..., None]
    result = lax.map(one_block, query_blocks)
    return result.reshape(length, -1)

def reference(tokens_in, norm_gain, window_query, window_key, window_value, window_query_gain, window_key_gain, sink_logit, dense_query, dense_key, dense_value, dense_query_gain, dense_key_gain, window_out, dense_out):
    inputs = tokens_in.astype(jnp.float32)
    normed = (inputs * lax.rsqrt(lax.optimization_barrier(jnp.mean(inputs * inputs, axis=-1, keepdims=True)) + EPS) * norm_gain).astype(jnp.bfloat16)

    def project(weight):
        return jnp.dot(normed, weight, preferred_element_type=jnp.float32)
    places = jnp.arange(TOKENS, dtype=jnp.int32)
    query_win = store(line_heads(project(window_query), window_query_gain, places))
    key_win = store(line_heads(project(window_key), window_key_gain, places))
    value_win = store(project(window_value))
    query_den = store(grid_heads(project(dense_query), dense_query_gain, places))
    key_den = store(grid_heads(project(dense_key), dense_key_gain, places))
    value_den = store(project(dense_value))
    margin = ((WINDOW, WINDOW), (0, 0))
    att_win = store(banded(query_win, jnp.pad(key_win, margin), jnp.pad(value_win, margin), 0, TOKENS, sink_logit))
    att_den = store(dense_attention(query_den, key_den, value_den))
    win_parts = att_win.reshape(TOKENS, N_TP, -1).transpose(1, 0, 2)
    den_parts = att_den.reshape(TOKENS, N_TP, -1).transpose(1, 0, 2)
    win_rows = window_out.reshape(N_TP, -1, D)
    den_rows = dense_out.reshape(N_TP, -1, D)

    def add_group(running, members):
        win_part, win_weight, den_part, den_weight = members
        partial_value = jnp.dot(win_part, win_weight, preferred_element_type=jnp.float32) + jnp.dot(den_part, den_weight, preferred_element_type=jnp.float32)
        return (running + store(partial_value).astype(jnp.float32), None)
    running, unused = lax.scan(add_group, jnp.zeros((TOKENS, D), jnp.float32), (win_parts, win_rows, den_parts, den_rows))
    return running.astype(jnp.bfloat16)
```

```python
import functools

import jax
import jax.numpy as jnp
import numpy as np
from jax import lax
from jax.experimental import pallas as pl
from jax.experimental.pallas import tpu as pltpu
from jax.sharding import PartitionSpec as P

HD = 64
WINDOW = 128
GRID_W = 64
EPS = 1e-06
THETA = 10000.0
MESH = pl.DeviceIdType.MESH
F32 = jnp.float32
BF16 = jnp.bfloat16
LOW = -1e30
OUT_EARLY = 4


def nt(a, b):
    return lax.dot_general(a, b, (((1,), (1,)), ((), ())), preferred_element_type=F32)


def nn(a, b):
    return jnp.dot(a, b, preferred_element_type=F32)


def remote(src, dst, send, recv, device):
    return pltpu.make_async_remote_copy(
        src_ref=src, dst_ref=dst, send_sem=send, recv_sem=recv, device_id=device, device_id_type=MESH
    )


class Ring:
    def __init__(self, me, n, piece, send_sem, recv_sem):
        self.me, self.n, self.half = me, n, n // 2
        self.piece, self.send_sem, self.recv_sem = piece, send_sem, recv_sem
        self.to = ({"sp": lax.rem(me + 1, n)}, {"sp": lax.rem(me + n - 1, n)})

    def owner(self, way, step):
        shift = self.n - step if way == 0 else step
        return lax.rem(self.me + shift, self.n)

    def copy(self, way, step, p):
        ref = self.piece(self.owner(way, step), p)
        return remote(
            ref, ref, self.send_sem.at[way, step, p], self.recv_sem.at[way, step, p], self.to[way]
        )

    def send(self, way, step, p):
        self.copy(way, step, p).start()

    def wait(self, way, step, p):
        ref = self.piece(self.owner(way, step + 1), p)
        remote(
            ref, ref, self.send_sem.at[way, step, p], self.recv_sem.at[way, step, p], self.to[way]
        ).wait_recv()

    def begin(self):
        for p in range(2):
            for way in range(2):
                self.send(way, 0, p)

    def hop_piece(self, step, p):
        for way in range(2):
            self.wait(way, step - 1, p)

            @pl.when((step < self.half - 1) | (p == way))
            def _():
                self.send(way, step, p)

    def hop(self, step):
        for p in range(2):
            self.hop_piece(step, p)

    def last(self):
        for way in range(2):
            self.wait(way, self.half - 1, way)

    def drain(self):
        def body(step, carry):
            for way in range(2):
                for p in range(2):
                    self.copy(way, step, p).wait_send()
            return carry

        lax.fori_loop(0, self.half - 1, body, 0)
        for way in range(2):
            self.copy(way, self.half - 1, way).wait_send()


def kernel(
    n_sp, n_tp,
    tokens, gain, wq, wk, wv, wqg, wkg, sink, dq, dk, dv, dqg, dkg, wo, do, freq,
    out,
    x, wall, stage, acc, oall, kv, kvw, qd, qw, att, attw, m_s, l_s, a_s,
    table, dsend, drecv, mine, xs, r2, c1, rc, rd,
    lsem, in_s, in_r, kv_s, kv_r, out_s, out_r, halo_s, halo_r,
    d_s, d_r, x_s, x_r,
):
    me = lax.axis_index("sp")
    tp = lax.axis_index("tp")
    core = lax.rem(tp, 2)
    xc = lax.div(tp, 2)
    n_x = n_tp // 2
    length, width = x.shape
    depth = wall.shape[1]
    cols = oall.shape[2]
    half_rows = length // 2
    share = length // n_tp
    half = n_sp // 2
    right, left = {"sp": lax.rem(me + 1, n_sp)}, {"sp": lax.rem(me + n_sp - 1, n_sp)}
    partner = {"tp": xc * 2 + (1 - core)}
    x_up = {"tp": lax.rem(xc + 1, n_x) * 2 + core}
    x_down = {"tp": lax.rem(xc + n_x - 1, n_x) * 2 + core}

    barrier = pltpu.get_barrier_semaphore()
    for peer in (right, left, partner, x_up, x_down):
        pl.semaphore_signal(barrier, inc=1, device_id=peer, device_id_type=MESH)

    loads = [
        pltpu.make_async_copy(wk, stage.at[0], lsem.at[0]),
        pltpu.make_async_copy(wv, stage.at[1], lsem.at[1]),
        pltpu.make_async_copy(dk, stage.at[2], lsem.at[2]),
        pltpu.make_async_copy(dv, stage.at[3], lsem.at[3]),
        pltpu.make_async_copy(wq, wall.at[me, :, pl.ds(0, 128)], lsem.at[4]),
        pltpu.make_async_copy(dq, wall.at[me, :, pl.ds(256, 128)], lsem.at[5]),
        pltpu.make_async_copy(wo, oall.at[me, pl.ds(0, 128)], lsem.at[6]),
        pltpu.make_async_copy(do, oall.at[me, pl.ds(128, 128)], lsem.at[7]),
    ]
    for c in loads:
        c.start()
    quarter = length // 4
    token_loads = [
        pltpu.make_async_copy(
            tokens.at[pl.ds(i * quarter, quarter)], x.at[pl.ds(i * quarter, quarter)], lsem.at[8 + i]
        )
        for i in range(4)
    ]
    for c in token_loads:
        c.start()
    for c in loads[:4]:
        c.wait()
    for at, base in ((0, 128), (2, 384)):
        pair = jnp.concatenate([stage[at], stage[at + 1]], axis=0).astype(F32)
        wall[me, :, base : base + 128] = pair.T.astype(BF16)
    for c in loads[4:]:
        c.wait()
    pl.semaphore_wait(barrier, 5)

    rows2 = depth // 2
    in_ring = Ring(me, n_sp, lambda w, p: wall.at[w, pl.ds(p * rows2, rows2)], in_s, in_r)
    out_ring = Ring(me, n_sp, lambda w, p: oall.at[w, pl.ds(p * 128, 128)], out_s, out_r)
    kv_rows = length // 2
    kv_ring = Ring(me, n_sp, lambda w, p: kv.at[w, pl.ds(p * kv_rows, kv_rows)], kv_s, kv_r)
    in_ring.begin()

    for i in range(4):
        token_loads[i].wait()

        def norm_rows(r, carry):
            at = pl.multiple_of(i * quarter + r * 16, 16)
            total = jnp.zeros((16, 128), F32)
            for j in range(width // 128):
                piece = x[pl.ds(at, 16), j * 128 : j * 128 + 128].astype(F32)
                total = total + piece * piece
            scale = lax.rsqrt(jnp.sum(total, axis=-1, keepdims=True) * (1.0 / width) + EPS)
            for j in range(width // 128):
                piece = x[pl.ds(at, 16), j * 128 : j * 128 + 128].astype(F32)
                x[pl.ds(at, 16), j * 128 : j * 128 + 128] = (
                    piece * scale * gain[j : j + 1, :]
                ).astype(BF16)
            return carry

        lax.fori_loop(0, quarter // 16, norm_rows, 0)

    lane = lax.broadcasted_iota(jnp.int32, (1, 128), 1)
    low_lane = lane < HD

    def tables(r, carry):
        at = pl.multiple_of(r * 64, 64)
        place = me * length + at + lax.broadcasted_iota(jnp.int32, (64, 128), 0)
        angle = place.astype(F32) * freq[0:1, :]
        table[0, pl.ds(at, 64)] = jnp.cos(angle)
        table[1, pl.ds(at, 64)] = jnp.sin(angle)
        row = lax.div(place, GRID_W)
        spot = jnp.where(lax.rem(lane, HD) < HD // 2, row, place - row * GRID_W)
        angle = spot.astype(F32) * freq[1:2, :]
        table[2, pl.ds(at, 64)] = jnp.cos(angle)
        table[3, pl.ds(at, 64)] = jnp.sin(angle)
        return carry

    lax.fori_loop(0, length // 64, tables, 0)

    def project(w, first=False):
        at = pl.multiple_of(w * depth, depth)
        product = nn(x[:, pl.ds(at, depth)], wall[w])
        if first:
            acc[...] = product
        else:
            acc[...] += product

    project(me, first=True)

    def in_step(d, carry):
        in_ring.hop(d)
        project(in_ring.owner(0, d))
        project(in_ring.owner(1, d))
        return carry

    lax.fori_loop(1, half, in_step, 0)
    out_ring.begin()
    in_ring.last()
    project(in_ring.owner(0, half))

    def two(ref):
        return jnp.concatenate([ref[...], ref[...]], axis=1)

    def heads(values, g, which, reach, rows):
        squares = values * values
        low = jnp.sum(jnp.where(low_lane, squares, 0.0), axis=-1, keepdims=True)
        high = jnp.sum(jnp.where(low_lane, 0.0, squares), axis=-1, keepdims=True)
        mean = jnp.where(low_lane, low, high) * (1.0 / HD)
        normed = values * lax.rsqrt(mean + EPS) * g
        turned = jnp.where(
            lax.rem(lane, 2 * reach) < reach,
            -pltpu.roll(normed, 128 - reach, 1),
            pltpu.roll(normed, reach, 1),
        )
        return normed * table[which, rows] + turned * table[which + 1, rows]

    blocks = [slice(i * 128, i * 128 + 128) for i in range(length // 128)]
    g = two(dkg)
    for rows in blocks:
        values = acc[rows, 384:512]
        kv[me, rows] = jnp.where(low_lane, heads(values, g, 2, HD // 4, rows), values).astype(BF16)
    g = two(wkg)
    for i, rows in enumerate(blocks):
        values = acc[rows, 128:256]
        kvw[pl.ds(WINDOW + i * 128, 128)] = jnp.where(
            low_lane, heads(values, g, 0, HD // 2, rows), values
        ).astype(BF16)
    kv_ring.begin()
    halos = [
        remote(
            kvw.at[pl.ds(length, WINDOW)], kvw.at[pl.ds(0, WINDOW)], halo_s.at[0], halo_r.at[0], right
        ),
        remote(
            kvw.at[pl.ds(WINDOW, WINDOW)],
            kvw.at[pl.ds(WINDOW + length, WINDOW)],
            halo_s.at[1],
            halo_r.at[1],
            left,
        ),
    ]
    for c in halos:
        c.start()
    scale = HD ** (-0.5)
    for ref, base, gain_ref, which, reach in ((qd, 256, dqg, 2, HD // 4), (qw, 0, wqg, 0, HD // 2)):
        g = two(gain_ref)
        for rows in blocks:
            q = heads(acc[rows, base : base + 128], g, which, reach, rows).astype(BF16).astype(F32)
            q = q * scale
            ref[0, rows] = jnp.where(low_lane, q, 0.0).astype(BF16)
            ref[1, rows] = jnp.where(low_lane, pltpu.roll(q, HD, 1), 0.0).astype(BF16)

    m_s[...] = jnp.full(m_s.shape, LOW, F32)
    l_s[...] = jnp.zeros(l_s.shape, F32)
    a_s[...] = jnp.zeros(a_s.shape, F32)

    for c in halos:
        c.wait_recv()

    def window(i):
        at = pl.multiple_of(i * 128, 128)
        queries = jnp.concatenate([qw[0, pl.ds(at, 128)], qw[1, pl.ds(at, 128)]], axis=0)
        near = kvw[pl.ds(at, 3 * WINDOW)]
        scores = nt(queries, near)
        row = lax.broadcasted_iota(jnp.int32, scores.shape, 0)
        key = lax.broadcasted_iota(jnp.int32, scores.shape, 1)
        first = row < 128
        spot = jnp.where(first, row, row - 128)
        place = me * length + at - WINDOW + key
        valid = (
            (key >= spot)
            & (key <= spot + 2 * WINDOW)
            & (place >= 0)
            & (place < length * n_sp)
        )
        scores = jnp.where(valid, scores, LOW)
        floor = jnp.where(
            lax.broadcasted_iota(jnp.int32, (256, 1), 0) < 128, sink[0], sink[1]
        )
        top = jnp.maximum(jnp.max(scores, axis=-1, keepdims=True), floor)
        expon = jnp.exp(scores - top)
        total = jnp.sum(expon, axis=-1, keepdims=True) + jnp.exp(floor - top)
        weights = (expon / total).astype(BF16)
        result = nn(weights, near)
        attw[0, pl.ds(at, 128)] = jnp.where(
            low_lane, pltpu.roll(result[:128], HD, 1), result[128:]
        ).astype(BF16)

    def dense(owners, j):
        rows = pl.ds(j * 256, 256)
        queries = qd_rows(j)
        scores = [nt(queries, kv[w]) for w in owners]
        before = m_s[rows]
        top = before
        for s in scores:
            top = jnp.maximum(top, jnp.max(s, axis=-1, keepdims=True))
        shrink = jnp.exp(before - top)
        expons = [jnp.exp(s - top[:, :1]) for s in scores]
        total = l_s[rows] * shrink
        summed = a_s[rows] * shrink
        for e, w in zip(expons, owners):
            total = total + jnp.sum(e, axis=-1, keepdims=True)
            summed = summed + nn(e.astype(BF16), kv[w])
        m_s[rows] = top
        l_s[rows] = total
        a_s[rows] = summed

    def qd_rows(j):
        flat = [qd[0, 0:256], None, qd[1, 128:384]]
        if j == 1:
            return jnp.concatenate([qd[0, 256:384], qd[1, 0:128]], axis=0)
        return flat[j]

    def kv_step(d, carry):
        before = d - 1

        @pl.when(d < half)
        def _():
            kv_ring.hop_piece(d, 0)

        @pl.when(d >= 2)
        def _():
            dense((kv_ring.owner(0, before), kv_ring.owner(1, before)), 0)

        @pl.when(d < half)
        def _():
            kv_ring.hop_piece(d, 1)

        @pl.when(d >= 2)
        def _():
            dense((kv_ring.owner(0, before), kv_ring.owner(1, before)), 1)

        @pl.when((lax.rem(d, 2) == 0) & (d <= 2 * OUT_EARLY))
        def _():
            out_ring.hop(lax.div(d, 2))

        @pl.when(d >= 2)
        def _():
            dense((kv_ring.owner(0, before), kv_ring.owner(1, before)), 2)

        @pl.when(d <= length // 128)
        def _():
            window(d - 1)

        return carry

    lax.fori_loop(1, half + 1, kv_step, 0)
    kv_ring.last()
    for j in range(3):
        dense((me, kv_ring.owner(0, half)), j)

    for rows in blocks:
        first = a_s[rows] / l_s[rows]
        second_rows = slice(rows.start + length, rows.stop + length)
        second = a_s[second_rows] / l_s[second_rows]
        attw[1, rows] = jnp.where(low_lane, pltpu.roll(first, HD, 1), second).astype(BF16)
    for t in range(n_tp):
        at = (t % 2) * half_rows + (t // 2) * share
        for which in range(2):
            att[at : at + share, which * 128 : which * 128 + 128] = attw[
                which, t * share : t * share + share
            ]

    def owners_of(s):
        return (
            lax.rem(me + n_sp - lax.rem(s, half), n_sp),
            lax.rem(me + s, n_sp),
        )

    theirs_at = pl.multiple_of((1 - core) * half_rows, half_rows)
    mine_at = pl.multiple_of(core * half_rows, half_rows)
    up = lax.rem(xc + 1, n_x)
    down = lax.rem(xc + n_x - 1, n_x)
    far = lax.rem(xc + 2, n_x)
    ways = ((x_up, up, x_down, down), (x_down, down, x_up, up))

    def pair_copy(s):
        return remote(dsend.at[s], drecv.at[s], d_s.at[s], d_r.at[s], partner)

    def far_copy(s, b):
        return remote(xs.at[s, b, far], r2.at[s, b], x_s.at[0, s, b], x_r.at[0, s, b], ways[b][0])

    def chain_copy(s, b):
        return remote(c1.at[s, b], rc.at[s, b], x_s.at[1, s, b], x_r.at[1, s, b], ways[b][0])

    def near_copy(s, b):
        return remote(
            xs.at[s, b, ways[b][3]], rd.at[s, b], x_s.at[2, s, b], x_r.at[2, s, b], ways[b][2]
        )

    def stage1(s):
        owners = owners_of(s)
        for b in range(2):
            dsend[s - 1, b] = nn(att[pl.ds(theirs_at, half_rows)], oall[owners[b]]).astype(BF16)
        mine[s - 1, 0] = nn(att[pl.ds(mine_at, half_rows)], oall[owners[0]])
        pair_copy(s - 1).start()
        mine[s - 1, 1] = nn(att[pl.ds(mine_at, half_rows)], oall[owners[1]])

    def stage2(s):
        pair_copy(s - 1).wait_recv()
        for b in range(2):
            both = (mine[s - 1, b] + drecv[s - 1, b].astype(F32)).astype(BF16)
            for t in range(n_x):
                xs[s - 1, b, t] = both[t * share : t * share + share]
        for b in range(2):
            far_copy(s - 1, b).start()
        for b in range(2):
            near_copy(s - 1, b).start()

    def stage3(s):
        for b in range(2):
            far_copy(s - 1, b).wait_recv()
            c1[s - 1, b] = (xs[s - 1, b, ways[b][1]].astype(F32) + r2[s - 1, b].astype(F32)).astype(
                BF16
            )
        for b in range(2):
            chain_copy(s - 1, b).start()

    def stage4(s):
        owners = owners_of(s)
        for b in range(2):
            chain_copy(s - 1, b).wait_recv()
            near_copy(s - 1, b).wait_recv()
            total = (
                xs[s - 1, b, xc].astype(F32) + rc[s - 1, b].astype(F32) + rd[s - 1, b].astype(F32)
            )
            at = pl.multiple_of(owners[b] * cols, cols)
            out[:, pl.ds(at, cols)] = total.astype(BF16)

    def out_step(s, carry):
        @pl.when((s > OUT_EARLY) & (s < half))
        def _():
            out_ring.hop(s)

        @pl.when(s == half)
        def _():
            out_ring.last()

        @pl.when(s <= half)
        def _():
            stage1(s)

        @pl.when((s >= 2) & (s <= half + 1))
        def _():
            stage2(s - 1)

        @pl.when((s >= 3) & (s <= half + 2))
        def _():
            stage3(s - 2)

        @pl.when(s >= 4)
        def _():
            stage4(s - 3)

        return carry

    lax.fori_loop(1, half + 4, out_step, 0)

    for ring in (in_ring, kv_ring, out_ring):
        ring.drain()
    for c in halos:
        c.wait_send()

    def drain(s, carry):
        pair_copy(s).wait_send()
        for b in range(2):
            far_copy(s, b).wait_send()
            near_copy(s, b).wait_send()
            chain_copy(s, b).wait_send()
        return carry

    lax.fori_loop(0, half, drain, 0)


def frequencies():
    lane = np.arange(128)
    line = THETA ** (-2.0 * (lane % (HD // 2)) / HD)
    grid = THETA ** (-2.0 * (lane % (HD // 4)) / (HD // 2))
    return np.stack([line, grid]).astype(np.float32)


def solution(mesh):
    n_sp, n_tp = mesh.shape["sp"], mesh.shape["tp"]
    assert n_sp % 2 == 0 and n_tp == 8

    def local(tokens, gain, wq, wk, wv, wqg, wkg, sink, dq, dk, dv, dqg, dkg, wo, do):
        length, width = tokens.shape
        depth, cols = wq.shape[0], wo.shape[1]
        half, n_x, share = n_sp // 2, n_tp // 2, length // n_tp
        assert wq.shape[1] == dq.shape[1] == 2 * HD and wk.shape[1] == dk.shape[1] == HD
        assert length % 128 == 0 and share % 16 == 0 and width == depth * n_sp
        any_, vmem = pl.BlockSpec(memory_space=pl.ANY), pl.BlockSpec(memory_space=pltpu.VMEM)
        smem = pl.BlockSpec(memory_space=pltpu.SMEM)
        dma = pltpu.SemaphoreType.DMA
        return pl.pallas_call(
            functools.partial(kernel, n_sp, n_tp),
            out_shape=jax.ShapeDtypeStruct((share, cols * n_sp), BF16),
            in_specs=[any_, vmem, any_, any_, any_, vmem, vmem, smem, any_, any_, any_, vmem, vmem, any_, any_, vmem],
            out_specs=vmem,
            scratch_shapes=[
                pltpu.VMEM((length, width), BF16),
                pltpu.VMEM((n_sp, depth, 512), BF16),
                pltpu.VMEM((4, HD, depth), BF16),
                pltpu.VMEM((length, 512), F32),
                pltpu.VMEM((n_sp, 256, cols), BF16),
                pltpu.VMEM((n_sp, length, 128), BF16),
                pltpu.VMEM((length + 2 * WINDOW, 128), BF16),
                pltpu.VMEM((2, length, 128), BF16),
                pltpu.VMEM((2, length, 128), BF16),
                pltpu.VMEM((length, 256), BF16),
                pltpu.VMEM((2, length, 128), BF16),
                pltpu.VMEM((2 * length, 128), F32),
                pltpu.VMEM((2 * length, 128), F32),
                pltpu.VMEM((2 * length, 128), F32),
                pltpu.VMEM((4, length, 128), F32),
                pltpu.VMEM((half, 2, length // 2, cols), BF16),
                pltpu.VMEM((half, 2, length // 2, cols), BF16),
                pltpu.VMEM((half, 2, length // 2, cols), F32),
                pltpu.VMEM((half, 2, n_x, share, cols), BF16),
                pltpu.VMEM((half, 2, share, cols), BF16),
                pltpu.VMEM((half, 2, share, cols), BF16),
                pltpu.VMEM((half, 2, share, cols), BF16),
                pltpu.VMEM((half, 2, share, cols), BF16),
                dma((12,)),
                dma((2, half, 2)),
                dma((2, half, 2)),
                dma((2, half, 2)),
                dma((2, half, 2)),
                dma((2, half, 2)),
                dma((2, half, 2)),
                dma((2,)),
                dma((2,)),
                dma((half,)),
                dma((half,)),
                dma((3, half, 2)),
                dma((3, half, 2)),
            ],
            compiler_params=pltpu.CompilerParams(
                collective_id=0, has_side_effects=True, vmem_limit_bytes=60 * 1024 * 1024
            ),
        )(
            tokens, gain.reshape(-1, 128), wq, wk.T, wv.T, wqg[None], wkg[None], sink,
            dq, dk.T, dv.T, dqg[None], dkg[None], wo, do, jnp.asarray(frequencies()),
        )

    return jax.shard_map(
        local,
        mesh=mesh,
        in_specs=(
            P(("grp", "sp"), None),
            P(),
            P("sp", "tp"),
            P("sp", "tp"),
            P("sp", "tp"),
            P(),
            P(),
            P("tp"),
            P("sp", "tp"),
            P("sp", "tp"),
            P("sp", "tp"),
            P(),
            P(),
            P("tp", "sp"),
            P("tp", "sp"),
        ),
        out_specs=P(("grp", "sp", "tp"), None),
        check_vma=False,
    )
```

```python
import functools
import math

import jax
import jax.numpy as jnp
import numpy as np
from jax import lax
from jax.experimental import pallas as pl
from jax.experimental.pallas import tpu as pltpu
from jax.sharding import PartitionSpec as P

HD = 64
WINDOW = 128
GRID_W = 64
EPS = 1e-06
THETA = 10000.0
MESH = pl.DeviceIdType.MESH
F32 = jnp.float32
BF16 = jnp.bfloat16
LOW = -1e30
OUT_EARLY = 8
LAG = (1, 3, 5)


def nt(a, b):
    return lax.dot_general(a, b, (((1,), (1,)), ((), ())), preferred_element_type=F32)


def nn(a, b):
    return jnp.dot(a, b, preferred_element_type=F32)


def remote(src, dst, send, recv, device):
    return pltpu.make_async_remote_copy(
        src_ref=src, dst_ref=dst, send_sem=send, recv_sem=recv, device_id=device, device_id_type=MESH
    )


class Ring:
    def __init__(self, me, n, piece, send_sem, recv_sem):
        self.me, self.n, self.half = me, n, n // 2
        self.piece, self.send_sem, self.recv_sem = piece, send_sem, recv_sem
        self.to = ({"sp": lax.rem(me + 1, n)}, {"sp": lax.rem(me + n - 1, n)})

    def owner(self, way, step):
        shift = self.n - step if way == 0 else step
        return lax.rem(self.me + shift, self.n)

    def copy(self, way, step, p):
        ref = self.piece(self.owner(way, step), p)
        return remote(
            ref, ref, self.send_sem.at[way, step, p], self.recv_sem.at[way, step, p], self.to[way]
        )

    def send(self, way, step, p):
        self.copy(way, step, p).start()

    def wait(self, way, step, p):
        ref = self.piece(self.owner(way, step + 1), p)
        remote(
            ref, ref, self.send_sem.at[way, step, p], self.recv_sem.at[way, step, p], self.to[way]
        ).wait_recv()

    def begin(self):
        for p in range(2):
            for way in range(2):
                self.send(way, 0, p)

    def hop_piece(self, step, p):
        for way in range(2):
            self.wait(way, step - 1, p)

            @pl.when((step < self.half - 1) | (p == way))
            def _():
                self.send(way, step, p)

    def hop(self, step):
        for p in range(2):
            self.hop_piece(step, p)

    def last(self):
        for way in range(2):
            self.wait(way, self.half - 1, way)

    def drain(self):
        def body(step, carry):
            for way in range(2):
                for p in range(2):
                    self.copy(way, step, p).wait_send()
            return carry

        lax.fori_loop(0, self.half - 1, body, 0)
        for way in range(2):
            self.copy(way, self.half - 1, way).wait_send()


class PairRing(Ring):
    def __init__(self, me, n, ref, give, side, other, send_sem, recv_sem, pair_send, pair_recv):
        rows = ref.shape[1]
        self.ref, self.give, self.other = ref, give, other
        self.given_at = pl.multiple_of(side * (rows - give), 16)
        self.taken_at = pl.multiple_of((1 - side) * (rows - give), 16)
        self.pair_send, self.pair_recv = pair_send, pair_recv

        def piece(w, p):
            return ref.at[w, pl.ds(self.given_at, give) if p == 0 else pl.ds(give, rows - 2 * give)]

        super().__init__(me, n, piece, send_sem, recv_sem)

    def across(self, way, step, at):
        ref = self.ref.at[self.owner(way, step), pl.ds(at, self.give)]
        return remote(
            ref, ref, self.pair_send.at[way, step - 1], self.pair_recv.at[way, step - 1], self.other
        )

    def hop_piece(self, step, p):
        super().hop_piece(step, p)
        if p == 0:
            for way in range(2):
                self.across(way, step, self.given_at).start()

    def last(self):
        self.wait(0, self.half - 1, 0)
        self.across(0, self.half, self.given_at).start()
        self.wait(1, self.half - 1, 1)

    def take(self, step):
        for way in range(2):
            self.across(way, step, self.taken_at).wait_recv()

    def take_last(self):
        self.across(0, self.half, self.taken_at).wait_recv()

    def drain(self):
        super().drain()

        def body(step, carry):
            for way in range(2):
                self.across(way, step, self.given_at).wait_send()
            return carry

        lax.fori_loop(1, self.half, body, 0)
        self.across(0, self.half, self.given_at).wait_send()


def kernel(
    n_sp, n_tp,
    tokens, gain, wq, wk, wv, wqg, wkg, sink, dq, dk, dv, dqg, dkg, wo, do, freq,
    out,
    x, wall, stage, acc, oall, kp, vt, kvw, qd, qw, att, attw, m_s, a_s,
    table, dsend, drecv, mine, xs, r2, c1, rc, rd,
    lsem, in_s, in_r, kv_s, kv_r, out_s, out_r, halo_s, halo_r,
    d_s, d_r, x_s, x_r, in_ys, in_yr, out_ys, out_yr, held, o_s,
):
    me = lax.axis_index("sp")
    tp = lax.axis_index("tp")
    core = lax.rem(tp, 2)
    xc = lax.div(tp, 2)
    n_x = n_tp // 2
    length, width = x.shape
    depth = wall.shape[1]
    cols = oall.shape[2]
    half_rows = length // 2
    share = length // n_tp
    half = n_sp // 2
    right, left = {"sp": lax.rem(me + 1, n_sp)}, {"sp": lax.rem(me + n_sp - 1, n_sp)}
    partner = {"tp": xc * 2 + (1 - core)}
    x_up = {"tp": lax.rem(xc + 1, n_x) * 2 + core}
    x_down = {"tp": lax.rem(xc + n_x - 1, n_x) * 2 + core}

    grp = lax.axis_index("grp")
    side = lax.rem(grp, 2)
    other = {"grp": grp + 1 - 2 * side}

    barrier = pltpu.get_barrier_semaphore()
    for peer in (right, left, partner, x_up, x_down, other):
        pl.semaphore_signal(barrier, inc=1, device_id=peer, device_id_type=MESH)

    loads = [
        pltpu.make_async_copy(wk, stage.at[0], lsem.at[0]),
        pltpu.make_async_copy(wv, stage.at[1], lsem.at[1]),
        pltpu.make_async_copy(dk, stage.at[2], lsem.at[2]),
        pltpu.make_async_copy(dv, stage.at[3], lsem.at[3]),
        pltpu.make_async_copy(wq, wall.at[me, :, pl.ds(0, 128)], lsem.at[4]),
        pltpu.make_async_copy(dq, wall.at[me, :, pl.ds(256, 128)], lsem.at[5]),
        pltpu.make_async_copy(wo, oall.at[me, pl.ds(0, 128)], lsem.at[6]),
        pltpu.make_async_copy(do, oall.at[me, pl.ds(128, 128)], lsem.at[7]),
    ]
    for c in loads:
        c.start()
    quarter = length // 4
    token_loads = [
        pltpu.make_async_copy(
            tokens.at[pl.ds(i * quarter, quarter)], x.at[pl.ds(i * quarter, quarter)], lsem.at[8 + i]
        )
        for i in range(4)
    ]
    for c in token_loads:
        c.start()
    for c in loads[:4]:
        c.wait()
    for at, base in ((0, 128), (2, 384)):
        pair = jnp.concatenate([stage[at], stage[at + 1]], axis=0).astype(F32)
        wall[me, :, base : base + 128] = pair.T.astype(BF16)
    for c in loads[4:]:
        c.wait()
    pl.semaphore_wait(barrier, 6)

    in_ring = PairRing(me, n_sp, wall, depth * 5 // 16, side, other, in_s, in_r, in_ys, in_yr)
    out_ring = PairRing(me, n_sp, oall, 80, side, other, out_s, out_r, out_ys, out_yr)
    kv_ring = Ring(me, n_sp, lambda w, p: (kp, vt)[p].at[w], kv_s, kv_r)
    in_ring.begin()

    def norm(i):
        token_loads[i].wait()

        def norm_rows(r, carry):
            at = pl.multiple_of(i * quarter + r * 16, 16)
            total = jnp.zeros((16, 128), F32)
            for j in range(width // 128):
                piece = x[pl.ds(at, 16), j * 128 : j * 128 + 128].astype(F32)
                total = total + piece * piece
            scale = lax.rsqrt(jnp.sum(total, axis=-1, keepdims=True) * (1.0 / width) + EPS)
            for j in range(width // 128):
                piece = x[pl.ds(at, 16), j * 128 : j * 128 + 128].astype(F32)
                x[pl.ds(at, 16), j * 128 : j * 128 + 128] = (
                    piece * scale * gain[j : j + 1, :]
                ).astype(BF16)
            return carry

        lax.fori_loop(0, quarter // 16, norm_rows, 0)

    lane = lax.broadcasted_iota(jnp.int32, (1, 128), 1)
    low_lane = lane < HD

    def tables(r, carry):
        at = pl.multiple_of(r * 64, 64)
        place = me * length + at + lax.broadcasted_iota(jnp.int32, (64, 128), 0)
        angle = place.astype(F32) * freq[0:1, :]
        table[0, pl.ds(at, 64)] = jnp.cos(angle)
        table[1, pl.ds(at, 64)] = jnp.sin(angle)
        row = lax.div(place, GRID_W)
        spot = jnp.where(lax.rem(lane, HD) < HD // 2, row, place - row * GRID_W)
        angle = spot.astype(F32) * freq[1:2, :]
        table[2, pl.ds(at, 64)] = jnp.cos(angle)
        table[3, pl.ds(at, 64)] = jnp.sin(angle)
        return carry

    def project(w, first=False):
        at = pl.multiple_of(w * depth, depth)
        product = nn(x[:, pl.ds(at, depth)], wall[w])
        if first:
            acc[...] = product
        else:
            acc[...] += product

    def projects(d, carry):
        in_ring.take(d)
        project(in_ring.owner(0, d))
        project(in_ring.owner(1, d))
        return carry

    def in_step(d, carry):
        in_ring.hop(d)

        @pl.when(d == 1)
        def _():
            norm(0)
            norm(1)

        @pl.when(d == 2)
        def _():
            norm(2)
            norm(3)

        @pl.when(d == 3)
        def _():
            lax.fori_loop(0, length // 64, tables, 0)
            project(me, first=True)

        @pl.when(d >= 4)
        def _():
            lax.fori_loop(
                jnp.where(d < 6, 2 * d - 7, d - 1), jnp.where(d < 6, 2 * d - 5, d), projects, 0
            )

        return carry

    lax.fori_loop(1, half, in_step, 0)
    out_ring.begin()
    in_ring.last()
    projects(half - 1, 0)
    in_ring.take_last()
    project(in_ring.owner(0, half))

    def two(ref):
        return jnp.concatenate([ref[...], ref[...]], axis=1)

    def heads(values, g, which, reach, rows):
        squares = values * values
        low = jnp.sum(jnp.where(low_lane, squares, 0.0), axis=-1, keepdims=True)
        high = jnp.sum(jnp.where(low_lane, 0.0, squares), axis=-1, keepdims=True)
        mean = jnp.where(low_lane, low, high) * (1.0 / HD)
        normed = values * lax.rsqrt(mean + EPS) * g
        turned = jnp.where(
            lax.rem(lane, 2 * reach) < reach,
            -pltpu.roll(normed, 128 - reach, 1),
            pltpu.roll(normed, reach, 1),
        )
        return normed * table[which, rows] + turned * table[which + 1, rows]

    blocks = [slice(i * 128, i * 128 + 128) for i in range(length // 128)]
    g = two(dkg)
    keys = [
        heads(acc[rows, 384:512], g, 2, HD // 4, rows)
        for rows in (slice(0, half_rows), slice(half_rows, length))
    ]
    kp[me] = jnp.where(low_lane, keys[0], pltpu.roll(keys[1], HD, 1)).astype(BF16)
    for rows in blocks:
        vt[me, :, rows] = acc[rows, 384:512].T[HD:].astype(BF16)
    g = two(wkg)
    for i, rows in enumerate(blocks):
        values = acc[rows, 128:256]
        kvw[pl.ds(WINDOW + i * 128, 128)] = jnp.where(
            low_lane, heads(values, g, 0, HD // 2, rows), values
        ).astype(BF16)
    kv_ring.begin()
    halos = [
        remote(
            kvw.at[pl.ds(length, WINDOW)], kvw.at[pl.ds(0, WINDOW)], halo_s.at[0], halo_r.at[0], right
        ),
        remote(
            kvw.at[pl.ds(WINDOW, WINDOW)],
            kvw.at[pl.ds(WINDOW + length, WINDOW)],
            halo_s.at[1],
            halo_r.at[1],
            left,
        ),
    ]
    for c in halos:
        c.start()
    scale = HD ** (-0.5)
    g = two(dqg)
    for rows in blocks:
        q = heads(acc[rows, 256:384], g, 2, HD // 4, rows) * (scale * math.log2(math.e))
        q = q.T.astype(BF16)
        for h in range(2):
            for p in range(2):
                cols_h = slice(h * length + rows.start, h * length + rows.stop)
                qd[p, p * HD : p * HD + HD, cols_h] = q[h * HD : h * HD + HD]
                qd[p, (1 - p) * HD : (1 - p) * HD + HD, cols_h] = jnp.zeros((HD, 128), BF16)
    g = two(wqg)
    for rows in blocks:
        q = heads(acc[rows, 0:128], g, 0, HD // 2, rows).astype(BF16).astype(F32) * scale
        qw[0, rows] = jnp.where(low_lane, q, 0.0).astype(BF16)
        qw[1, rows] = jnp.where(low_lane, pltpu.roll(q, HD, 1), 0.0).astype(BF16)

    m_s[...] = jnp.full(m_s.shape, LOW, F32)
    a_s[...] = jnp.zeros(a_s.shape, F32)

    def window(i):
        at = pl.multiple_of(i * 128, 128)
        queries = jnp.concatenate([qw[0, pl.ds(at, 128)], qw[1, pl.ds(at, 128)]], axis=0)
        near = kvw[pl.ds(at, 3 * WINDOW)]
        scores = nt(queries, near)
        row = lax.broadcasted_iota(jnp.int32, scores.shape, 0)
        key = lax.broadcasted_iota(jnp.int32, scores.shape, 1)
        first = row < 128
        spot = jnp.where(first, row, row - 128)
        place = me * length + at - WINDOW + key
        valid = (
            (key >= spot)
            & (key <= spot + 2 * WINDOW)
            & (place >= 0)
            & (place < length * n_sp)
        )
        scores = jnp.where(valid, scores, LOW)
        floor = jnp.where(
            lax.broadcasted_iota(jnp.int32, (256, 1), 0) < 128, sink[0], sink[1]
        )
        top = jnp.maximum(jnp.max(scores, axis=-1, keepdims=True), floor)
        expon = jnp.exp(scores - top)
        total = jnp.sum(expon, axis=-1, keepdims=True) + jnp.exp(floor - top)
        weights = (expon / total).astype(BF16)
        result = nn(weights, near)
        attw[0, pl.ds(at, 128)] = jnp.where(
            low_lane, pltpu.roll(result[:128], HD, 1), result[128:]
        ).astype(BF16)

    ones = jnp.ones((8, 2 * length), BF16)

    def dense(owners):
        keys = jnp.concatenate([kp[w] for w in owners], axis=0)
        values = jnp.concatenate(
            [jnp.concatenate([vt[w] for w in owners], axis=1), ones], axis=0
        )
        low, high = nn(keys, qd[0]), nn(keys, qd[1])
        before = m_s[...]
        top = jnp.maximum(before, jnp.max(jnp.maximum(low, high), axis=0, keepdims=True))
        shrink = jnp.exp2(before - top)
        low = jnp.exp2(low - top[:1]).astype(BF16)
        high = jnp.exp2(high - top[:1]).astype(BF16)
        expons = jnp.concatenate(
            [low[:half_rows], high[:half_rows], low[half_rows:], high[half_rows:]], axis=0
        )
        a_s[...] = a_s[...] * shrink[:1] + nn(values, expons)
        m_s[...] = top

    def kv_step(d, carry):
        @pl.when(d < half)
        def _():
            kv_ring.hop(d)

        @pl.when((d <= OUT_EARLY) & (d < half))
        def _():
            out_ring.hop(d)

        @pl.when((d == OUT_EARLY) & (d == half))
        def _():
            out_ring.last()

        @pl.when(d >= 2)
        def _():
            dense((kv_ring.owner(0, d - 1), kv_ring.owner(1, d - 1)))

        @pl.when(d == 3)
        def _():
            for c in halos:
                c.wait_recv()

        @pl.when((d >= 3) & (d < 3 + length // 128))
        def _():
            window(d - 3)

        return carry

    lax.fori_loop(1, half + 1, kv_step, 0)
    kv_ring.last()
    dense((me, kv_ring.owner(0, half)))
    both = jnp.concatenate(
        [a_s[:HD, h * length : h * length + length] / a_s[HD : HD + 1, h * length : h * length + length] for h in range(2)],
        axis=0,
    )
    for rows in blocks:
        attw[1, rows] = both[:, rows].T.astype(BF16)
    for t in range(n_tp):
        at = (t % 2) * half_rows + (t // 2) * share
        for which in range(2):
            att[at : at + share, which * 128 : which * 128 + 128] = attw[
                which, t * share : t * share + share
            ]

    def owners_of(s):
        return (
            lax.rem(me + n_sp - lax.rem(s, half), n_sp),
            lax.rem(me + s, n_sp),
        )

    theirs_at = pl.multiple_of((1 - core) * half_rows, half_rows)
    mine_at = pl.multiple_of(core * half_rows, half_rows)
    up = lax.rem(xc + 1, n_x)
    down = lax.rem(xc + n_x - 1, n_x)
    far = lax.rem(xc + 2, n_x)
    ways = ((x_up, up, x_down, down), (x_down, down, x_up, up))

    def pair_copy(s):
        return remote(dsend.at[s], drecv.at[s], d_s.at[s], d_r.at[s], partner)

    def far_copy(s, b):
        return remote(xs.at[s, b, far], r2.at[s, b], x_s.at[0, s, b], x_r.at[0, s, b], ways[b][0])

    def chain_copy(s, b):
        return remote(c1.at[s, b], rc.at[s, b], x_s.at[1, s, b], x_r.at[1, s, b], ways[b][0])

    def near_copy(s, b):
        return remote(
            xs.at[s, b, ways[b][3]], rd.at[s, b], x_s.at[2, s, b], x_r.at[2, s, b], ways[b][2]
        )

    def put(s, b):
        at = pl.multiple_of(owners_of(s)[b] * cols, cols)
        return pltpu.make_async_copy(held.at[s - 1, b], out.at[:, pl.ds(at, cols)], o_s.at[s - 1, b])

    def stage1(s):
        owners = owners_of(s)
        for b in range(2):
            dsend[s - 1, b] = nn(att[pl.ds(theirs_at, half_rows)], oall[owners[b]]).astype(BF16)
        mine[s - 1, 0] = nn(att[pl.ds(mine_at, half_rows)], oall[owners[0]])
        pair_copy(s - 1).start()
        mine[s - 1, 1] = nn(att[pl.ds(mine_at, half_rows)], oall[owners[1]])

    def stage2(s):
        pair_copy(s - 1).wait_recv()
        for b in range(2):
            both = (mine[s - 1, b] + drecv[s - 1, b].astype(F32)).astype(BF16)
            for t in range(n_x):
                xs[s - 1, b, t] = both[t * share : t * share + share]
        for b in range(2):
            far_copy(s - 1, b).start()
        for b in range(2):
            near_copy(s - 1, b).start()

    def stage3(s):
        for b in range(2):
            far_copy(s - 1, b).wait_recv()
            c1[s - 1, b] = (xs[s - 1, b, ways[b][1]].astype(F32) + r2[s - 1, b].astype(F32)).astype(
                BF16
            )
        for b in range(2):
            chain_copy(s - 1, b).start()

    def stage4(s):
        for b in range(2):
            chain_copy(s - 1, b).wait_recv()
            near_copy(s - 1, b).wait_recv()
            total = (
                xs[s - 1, b, xc].astype(F32) + rc[s - 1, b].astype(F32) + rd[s - 1, b].astype(F32)
            )
            held[s - 1, b] = total.astype(BF16)
        for b in range(2):
            put(s, b).start()

    def out_step(s, carry):
        ahead = s + OUT_EARLY

        @pl.when(ahead < half)
        def _():
            out_ring.hop(ahead)

        @pl.when(ahead == half)
        def _():
            out_ring.last()

        @pl.when(s < half)
        def _():
            out_ring.take(s)

        @pl.when(s == half)
        def _():
            out_ring.take_last()

        @pl.when(s <= half)
        def _():
            stage1(s)

        @pl.when((s >= 1 + LAG[0]) & (s <= half + LAG[0]))
        def _():
            stage2(s - LAG[0])

        @pl.when((s >= 1 + LAG[1]) & (s <= half + LAG[1]))
        def _():
            stage3(s - LAG[1])

        @pl.when(s >= 1 + LAG[2])
        def _():
            stage4(s - LAG[2])

        @pl.when(s == 3)
        def _():
            in_ring.drain()
            kv_ring.drain()
            for c in halos:
                c.wait_send()

        return carry

    lax.fori_loop(1, half + LAG[2] + 1, out_step, 0)

    out_ring.drain()

    def drain(s, carry):
        pair_copy(s).wait_send()
        for b in range(2):
            far_copy(s, b).wait_send()
            near_copy(s, b).wait_send()
            chain_copy(s, b).wait_send()
            put(s + 1, b).wait()
        return carry

    lax.fori_loop(0, half, drain, 0)


def frequencies():
    lane = np.arange(128)
    line = THETA ** (-2.0 * (lane % (HD // 2)) / HD)
    grid = THETA ** (-2.0 * (lane % (HD // 4)) / (HD // 2))
    return np.stack([line, grid]).astype(np.float32)


def solution(mesh):
    n_sp, n_tp = mesh.shape["sp"], mesh.shape["tp"]
    assert n_sp % 2 == 0 and n_tp == 8 and mesh.shape["grp"] % 2 == 0

    def local(tokens, gain, wq, wk, wv, wqg, wkg, sink, dq, dk, dv, dqg, dkg, wo, do):
        length, width = tokens.shape
        depth, cols = wq.shape[0], wo.shape[1]
        half, n_x, share = n_sp // 2, n_tp // 2, length // n_tp
        assert wq.shape[1] == dq.shape[1] == 2 * HD and wk.shape[1] == dk.shape[1] == HD
        assert length % 128 == 0 and share % 16 == 0 and width == depth * n_sp
        any_, vmem = pl.BlockSpec(memory_space=pl.ANY), pl.BlockSpec(memory_space=pltpu.VMEM)
        smem = pl.BlockSpec(memory_space=pltpu.SMEM)
        dma = pltpu.SemaphoreType.DMA
        return pl.pallas_call(
            functools.partial(kernel, n_sp, n_tp),
            out_shape=jax.ShapeDtypeStruct((share, cols * n_sp), BF16),
            in_specs=[any_, vmem, any_, any_, any_, vmem, vmem, smem, any_, any_, any_, vmem, vmem, any_, any_, vmem],
            out_specs=any_,
            scratch_shapes=[
                pltpu.VMEM((length, width), BF16),
                pltpu.VMEM((n_sp, depth, 512), BF16),
                pltpu.VMEM((4, HD, depth), BF16),
                pltpu.VMEM((length, 512), F32),
                pltpu.VMEM((n_sp, 256, cols), BF16),
                pltpu.VMEM((n_sp, length // 2, 128), BF16),
                pltpu.VMEM((n_sp, HD, length), BF16),
                pltpu.VMEM((length + 2 * WINDOW, 128), BF16),
                pltpu.VMEM((2, 128, 2 * length), BF16),
                pltpu.VMEM((2, length, 128), BF16),
                pltpu.VMEM((length, 256), BF16),
                pltpu.VMEM((2, length, 128), BF16),
                pltpu.VMEM((8, 2 * length), F32),
                pltpu.VMEM((HD + 8, 2 * length), F32),
                pltpu.VMEM((4, length, 128), F32),
                pltpu.VMEM((half, 2, length // 2, cols), BF16),
                pltpu.VMEM((half, 2, length // 2, cols), BF16),
                pltpu.VMEM((half, 2, length // 2, cols), F32),
                pltpu.VMEM((half, 2, n_x, share, cols), BF16),
                pltpu.VMEM((half, 2, share, cols), BF16),
                pltpu.VMEM((half, 2, share, cols), BF16),
                pltpu.VMEM((half, 2, share, cols), BF16),
                pltpu.VMEM((half, 2, share, cols), BF16),
                dma((12,)),
                dma((2, half, 2)),
                dma((2, half, 2)),
                dma((2, half, 2)),
                dma((2, half, 2)),
                dma((2, half, 2)),
                dma((2, half, 2)),
                dma((2,)),
                dma((2,)),
                dma((half,)),
                dma((half,)),
                dma((3, half, 2)),
                dma((3, half, 2)),
                dma((2, half)),
                dma((2, half)),
                dma((2, half)),
                dma((2, half)),
                pltpu.VMEM((half, 2, share, cols), BF16),
                dma((half, 2)),
            ],
            compiler_params=pltpu.CompilerParams(
                collective_id=0, has_side_effects=True, vmem_limit_bytes=60 * 1024 * 1024
            ),
        )(
            tokens, gain.reshape(-1, 128), wq, wk.T, wv.T, wqg[None], wkg[None], sink,
            dq, dk.T, dv.T, dqg[None], dkg[None], wo, do, jnp.asarray(frequencies()),
        )

    return jax.shard_map(
        local,
        mesh=mesh,
        in_specs=(
            P(("grp", "sp"), None),
            P(),
            P("sp", "tp"),
            P("sp", "tp"),
            P("sp", "tp"),
            P(),
            P(),
            P("tp"),
            P("sp", "tp"),
            P("sp", "tp"),
            P("sp", "tp"),
            P(),
            P(),
            P("tp", "sp"),
            P("tp", "sp"),
        ),
        out_specs=P(("grp", "sp", "tp"), None),
        check_vma=False,
    )
```

```python
import functools
import math

import jax
import jax.numpy as jnp
import numpy as np
from jax import lax
from jax.experimental import pallas as pl
from jax.experimental.pallas import tpu as pltpu
from jax.sharding import PartitionSpec as P

HD = 64
WINDOW = 128
GRID_W = 64
EPS = 1e-06
THETA = 10000.0
MESH = pl.DeviceIdType.MESH
F32 = jnp.float32
BF16 = jnp.bfloat16
LOW = -1e30
LAG = (1, 5, 2, 13)


def nt(a, b):
    return lax.dot_general(a, b, (((1,), (1,)), ((), ())), preferred_element_type=F32)


def nn(a, b):
    return jnp.dot(a, b, preferred_element_type=F32)


def remote(src, dst, send, recv, device):
    return pltpu.make_async_remote_copy(
        src_ref=src, dst_ref=dst, send_sem=send, recv_sem=recv, device_id=device, device_id_type=MESH
    )


class Ring:
    def __init__(self, me, n, count, piece, send_sem, recv_sem, place=0):
        self.place = place
        self.me, self.n, self.half = me, n, n // 2
        self.count = count
        self.piece, self.send_sem, self.recv_sem = piece, send_sem, recv_sem
        self.to = ({"sp": lax.rem(me + 1, n)}, {"sp": lax.rem(me + n - 1, n)})

    def owner(self, way, step):
        shift = self.n - step if way == 0 else step
        return lax.rem(self.me + shift, self.n)

    def copy(self, way, step, p, distance):
        ref = self.piece(self.owner(way, distance), p)
        return remote(
            ref, ref, self.send_sem.at[way, lax.rem(step, 2), p], self.recv_sem.at[way, step, self.place + p], self.to[way]
        )

    def send(self, way, step, p):
        @pl.when(step >= 2)
        def _():
            self.copy(way, step - 2, p, step - 2).wait_send()

        self.copy(way, step, p, step).start()

    def wait(self, way, step, p):
        self.copy(way, step, p, step + 1).wait_recv()

    def way_of(self, p):
        return 2 * p // self.count

    def begin(self):
        for p in range(self.count):
            for way in range(2):
                self.copy(way, 0, p, 0).start()

    def hop_piece(self, step, p):
        for way in range(2):
            self.wait(way, step - 1, p)

            @pl.when((step < self.half - 1) | (self.way_of(p) == way))
            def _():
                self.send(way, step, p)

    def wait_last(self, way):
        for p in range(self.count):
            if self.way_of(p) == way:
                self.wait(way, self.half - 1, p)

    def last(self):
        for way in range(2):
            self.wait_last(way)

    def drain(self):
        for way in range(2):
            for p in range(self.count):
                final = self.half - 1 if self.way_of(p) == way else self.half - 2
                for step in (final - 1, final):
                    self.copy(way, step, p, step).wait_send()


class PairRing(Ring):
    def __init__(self, me, n, ref, give, side, other, send_sem, recv_sem, pair_send, pair_recv):
        rows = ref.shape[1]
        common = rows - 2 * give
        self.ref, self.give, self.other = ref, give, other
        self.given_at = pl.multiple_of(side * (rows - give), 16)
        self.taken_at = pl.multiple_of((1 - side) * (rows - give), 16)
        self.pair_send, self.pair_recv = pair_send, pair_recv
        if common:
            first = give // 32 * 16
            cuts = [(0, first), (first, give - first)]
            later = [(give, common // 2), (give + common // 2, common - common // 2)]
        else:
            cuts, later = [(0, give // 2), (give // 2, give // 2)], []
        self.cross_after = 1
        self.early_cross = bool(later)

        def piece(w, p):
            if p < 2:
                at = pl.multiple_of(self.given_at + cuts[p][0], 16)
                return ref.at[w, pl.ds(at, cuts[p][1])]
            return ref.at[w, pl.ds(*later[p - 2])]

        super().__init__(me, n, 2 + len(later), piece, send_sem, recv_sem, 0 if later else 2)

    def across(self, way, step, at):
        ref = self.ref.at[self.owner(way, step), pl.ds(at, self.give)]
        return remote(
            ref, ref, self.pair_send.at[way, lax.rem(step, 2)], self.pair_recv.at[way, step - 1], self.other
        )

    def hop_piece(self, step, p):
        super().hop_piece(step, p)
        if p == self.cross_after:
            for way in range(2):

                @pl.when(step >= 3)
                def _():
                    self.across(way, step - 2, self.given_at).wait_send()

                self.across(way, step, self.given_at).start()

    def last_first(self):
        self.wait_last(0)
        if not self.early_cross:
            self.wait_last(1)
        self.across(0, self.half - 2, self.given_at).wait_send()
        self.across(0, self.half, self.given_at).start()

    def last_second(self):
        if self.early_cross:
            self.wait_last(1)

    def last(self):
        self.last_first()
        self.last_second()

    def take(self, step):
        for way in range(2):
            self.across(way, step, self.taken_at).wait_recv()

    def take_last(self):
        self.across(0, self.half, self.taken_at).wait_recv()

    def drain(self):
        super().drain()
        self.across(0, self.half, self.given_at).wait_send()
        for way in range(2):
            self.across(way, self.half - 1, self.given_at).wait_send()
        self.across(1, self.half - 2, self.given_at).wait_send()


def kernel(
    n_sp, n_tp,
    tokens, gain_h, wq, wk, wv, wqg_h, wkg_h, sink, dq, dk, dv, dqg_h, dkg_h, wo, do, freq_h,
    out,
    x, wall, stage, acc, oall, kp, vt, kvw, qd, qw, att, attw, m_s, a_s,
    table, dsend, drecv, mine, xs, r2, c1, rc, rd,
    lsem, in_s, in_r, out_s, halo_s, halo_r,
    d_s, d_r, x_s, x_r, in_ys, in_yr, out_ys, out_yr, held, o_s,
    gain, gains, freq, kv_snd,
):
    me = lax.axis_index("sp")
    tp = lax.axis_index("tp")
    core = lax.rem(tp, 2)
    xc = lax.div(tp, 2)
    n_x = n_tp // 2
    length, width = x.shape
    depth = wall.shape[1]
    cols = oall.shape[2]
    half_rows = length // 2
    share = length // n_tp
    half = n_sp // 2
    right, left = {"sp": lax.rem(me + 1, n_sp)}, {"sp": lax.rem(me + n_sp - 1, n_sp)}
    partner = {"tp": xc * 2 + (1 - core)}
    x_up = {"tp": lax.rem(xc + 1, n_x) * 2 + core}
    x_down = {"tp": lax.rem(xc + n_x - 1, n_x) * 2 + core}

    grp = lax.axis_index("grp")
    side = lax.rem(grp, 2)
    other = {"grp": grp + 1 - 2 * side}

    barrier = pltpu.get_barrier_semaphore()
    for peer in (right, left, partner, x_up, x_down, other):
        pl.semaphore_signal(barrier, inc=1, device_id=peer, device_id_type=MESH)

    loads = [
        pltpu.make_async_copy(wk, stage.at[0], lsem.at[0]),
        pltpu.make_async_copy(wv, stage.at[1], lsem.at[1]),
        pltpu.make_async_copy(dk, stage.at[2], lsem.at[2]),
        pltpu.make_async_copy(dv, stage.at[3], lsem.at[3]),
        pltpu.make_async_copy(wq, wall.at[me, :, pl.ds(0, 128)], lsem.at[4]),
        pltpu.make_async_copy(dq, wall.at[me, :, pl.ds(256, 128)], lsem.at[5]),
        pltpu.make_async_copy(wo, oall.at[me, pl.ds(0, 128)], lsem.at[6]),
        pltpu.make_async_copy(do, oall.at[me, pl.ds(128, 128)], lsem.at[7]),
    ]
    small = [
        pltpu.make_async_copy(src, dst, lsem.at[12 + i])
        for i, (src, dst) in enumerate(
            [(gain_h, gain), (freq_h, freq)]
            + [(g, gains.at[j]) for j, g in enumerate((wqg_h, wkg_h, dqg_h, dkg_h))]
        )
    ]
    for c in loads:
        c.start()
    quarter = length // 4
    token_loads = [
        pltpu.make_async_copy(
            tokens.at[pl.ds(i * quarter, quarter)], x.at[pl.ds(i * quarter, quarter)], lsem.at[8 + i]
        )
        for i in range(4)
    ]
    for c in token_loads + small:
        c.start()
    for c in loads[:4]:
        c.wait()
    for at, base in ((0, 128), (2, 384)):
        pair = jnp.concatenate([stage[at], stage[at + 1]], axis=0).astype(F32)
        wall[me, :, base : base + 128] = pair.T.astype(BF16)
    for c in loads[4:]:
        c.wait()
    pl.semaphore_wait(barrier, 6)

    in_ring = PairRing(me, n_sp, wall, depth * 5 // 16, side, other, in_s, in_r, in_ys, in_yr)
    out_ring = PairRing(me, n_sp, oall, 128, side, other, out_s, in_r, out_ys, out_yr)
    kv_ring = Ring(me, n_sp, 2, lambda w, p: (kp, vt)[p].at[w], kv_snd, in_r)
    in_ring.begin()
    for c in small:
        c.wait()

    def norm(i):
        token_loads[i].wait()

        def norm_rows(r, carry):
            at = pl.multiple_of(i * quarter + r * 16, 16)
            total = jnp.zeros((16, 128), F32)
            for j in range(width // 128):
                piece = x[pl.ds(at, 16), j * 128 : j * 128 + 128].astype(F32)
                total = total + piece * piece
            scale = lax.rsqrt(jnp.sum(total, axis=-1, keepdims=True) * (1.0 / width) + EPS)
            for j in range(width // 128):
                piece = x[pl.ds(at, 16), j * 128 : j * 128 + 128].astype(F32)
                x[pl.ds(at, 16), j * 128 : j * 128 + 128] = (
                    piece * scale * gain[j : j + 1, :]
                ).astype(BF16)
            return carry

        lax.fori_loop(0, quarter // 16, norm_rows, 0)

    lane = lax.broadcasted_iota(jnp.int32, (1, 128), 1)
    low_lane = lane < HD

    def tables(r, carry):
        at = pl.multiple_of(r * 64, 64)
        place = me * length + at + lax.broadcasted_iota(jnp.int32, (64, 128), 0)
        angle = place.astype(F32) * freq[0:1, :]
        table[0, pl.ds(at, 64)] = jnp.cos(angle)
        table[1, pl.ds(at, 64)] = jnp.sin(angle)
        row = lax.div(place, GRID_W)
        spot = jnp.where(lax.rem(lane, HD) < HD // 2, row, place - row * GRID_W)
        angle = spot.astype(F32) * freq[1:2, :]
        table[2, pl.ds(at, 64)] = jnp.cos(angle)
        table[3, pl.ds(at, 64)] = jnp.sin(angle)
        return carry

    def project(w, first=False):
        at = pl.multiple_of(w * depth, depth)
        product = nn(x[:, pl.ds(at, depth)], wall[w])
        if first:
            acc[...] = product
        else:
            acc[...] += product

    def projects(d, carry):
        in_ring.take(d)
        project(in_ring.owner(0, d))
        project(in_ring.owner(1, d))
        return carry

    def in_step(d, carry):
        in_ring.hop_piece(d, 0)
        in_ring.hop_piece(d, 1)

        @pl.when(d == 1)
        def _():
            norm(0)
            norm(1)

        @pl.when(d == 2)
        def _():
            norm(2)
            norm(3)

        @pl.when(d == 3)
        def _():
            lax.fori_loop(0, length // 64, tables, 0)
            project(me, first=True)

        @pl.when(d >= 4)
        def _():
            lax.fori_loop(jnp.where(d == 4, 1, d - 2), d - 1, projects, 0)

        in_ring.hop_piece(d, 2)
        in_ring.hop_piece(d, 3)
        return carry

    lax.fori_loop(1, half, in_step, 0)
    out_ring.begin()
    projects(half - 2, 0)
    in_ring.last_first()
    projects(half - 1, 0)
    in_ring.last_second()
    in_ring.take_last()
    project(in_ring.owner(0, half))

    def two(which):
        return jnp.concatenate([gains[which], gains[which]], axis=1)

    def heads(values, g, which, reach, rows):
        squares = values * values
        low = jnp.sum(jnp.where(low_lane, squares, 0.0), axis=-1, keepdims=True)
        high = jnp.sum(jnp.where(low_lane, 0.0, squares), axis=-1, keepdims=True)
        mean = jnp.where(low_lane, low, high) * (1.0 / HD)
        normed = values * lax.rsqrt(mean + EPS) * g
        turned = jnp.where(
            lax.rem(lane, 2 * reach) < reach,
            -pltpu.roll(normed, 128 - reach, 1),
            pltpu.roll(normed, reach, 1),
        )
        return normed * table[which, rows] + turned * table[which + 1, rows]

    blocks = [slice(i * 128, i * 128 + 128) for i in range(length // 128)]
    g = two(3)
    keys = [
        heads(acc[rows, 384:512], g, 2, HD // 4, rows)
        for rows in (slice(0, half_rows), slice(half_rows, length))
    ]
    kp[me] = jnp.where(low_lane, keys[0], pltpu.roll(keys[1], HD, 1)).astype(BF16)
    for rows in blocks:
        vt[me, :, rows] = acc[rows, 384:512].T[HD:].astype(BF16)
    g = two(1)
    for i, rows in enumerate(blocks):
        values = acc[rows, 128:256]
        kvw[pl.ds(WINDOW + i * 128, 128)] = jnp.where(
            low_lane, heads(values, g, 0, HD // 2, rows), values
        ).astype(BF16)
    kv_ring.begin()
    halos = [
        remote(
            kvw.at[pl.ds(length, WINDOW)], kvw.at[pl.ds(0, WINDOW)], halo_s.at[0], halo_r.at[0], right
        ),
        remote(
            kvw.at[pl.ds(WINDOW, WINDOW)],
            kvw.at[pl.ds(WINDOW + length, WINDOW)],
            halo_s.at[1],
            halo_r.at[1],
            left,
        ),
    ]
    for c in halos:
        c.start()
    scale = HD ** (-0.5)
    g = two(2)
    for rows in blocks:
        q = heads(acc[rows, 256:384], g, 2, HD // 4, rows) * (scale * math.log2(math.e))
        q = q.T.astype(BF16)
        for h in range(2):
            for p in range(2):
                cols_h = slice(h * length + rows.start, h * length + rows.stop)
                qd[p, p * HD : p * HD + HD, cols_h] = q[h * HD : h * HD + HD]
                qd[p, (1 - p) * HD : (1 - p) * HD + HD, cols_h] = jnp.zeros((HD, 128), BF16)
    g = two(0)
    for rows in blocks:
        q = heads(acc[rows, 0:128], g, 0, HD // 2, rows).astype(BF16).astype(F32) * scale
        qw[0, rows] = jnp.where(low_lane, q, 0.0).astype(BF16)
        qw[1, rows] = jnp.where(low_lane, pltpu.roll(q, HD, 1), 0.0).astype(BF16)

    m_s[...] = jnp.full(m_s.shape, LOW, F32)
    a_s[...] = jnp.zeros(a_s.shape, F32)

    def window(i):
        at = pl.multiple_of(i * 128, 128)
        queries = jnp.concatenate([qw[0, pl.ds(at, 128)], qw[1, pl.ds(at, 128)]], axis=0)
        near = kvw[pl.ds(at, 3 * WINDOW)]
        scores = nt(queries, near)
        row = lax.broadcasted_iota(jnp.int32, scores.shape, 0)
        key = lax.broadcasted_iota(jnp.int32, scores.shape, 1)
        first = row < 128
        spot = jnp.where(first, row, row - 128)
        place = me * length + at - WINDOW + key
        valid = (
            (key >= spot)
            & (key <= spot + 2 * WINDOW)
            & (place >= 0)
            & (place < length * n_sp)
        )
        scores = jnp.where(valid, scores, LOW)
        floor = jnp.where(
            lax.broadcasted_iota(jnp.int32, (256, 1), 0) < 128, sink[0], sink[1]
        )
        top = jnp.maximum(jnp.max(scores, axis=-1, keepdims=True), floor)
        expon = jnp.exp(scores - top)
        total = jnp.sum(expon, axis=-1, keepdims=True) + jnp.exp(floor - top)
        weights = (expon / total).astype(BF16)
        result = nn(weights, near)
        attw[0, pl.ds(at, 128)] = jnp.where(
            low_lane, pltpu.roll(result[:128], HD, 1), result[128:]
        ).astype(BF16)

    ones = jnp.ones((8, 2 * length), BF16)

    def dense(owners):
        keys = jnp.concatenate([kp[w] for w in owners], axis=0)
        values = jnp.concatenate(
            [jnp.concatenate([vt[w] for w in owners], axis=1), ones], axis=0
        )
        low, high = nn(keys, qd[0]), nn(keys, qd[1])
        before = m_s[...]
        top = jnp.maximum(before, jnp.max(jnp.maximum(low, high), axis=0, keepdims=True))
        shrink = jnp.exp2(before - top)
        low = jnp.exp2(low - top[:1]).astype(BF16)
        high = jnp.exp2(high - top[:1]).astype(BF16)
        expons = jnp.concatenate(
            [low[:half_rows], high[:half_rows], low[half_rows:], high[half_rows:]], axis=0
        )
        a_s[...] = a_s[...] * shrink[:1] + nn(values, expons)
        m_s[...] = top

    def kv_step(d, carry):
        @pl.when(d < half)
        def _():
            kv_ring.hop_piece(d, 0)
            kv_ring.hop_piece(d, 1)

        @pl.when((d + 1 < half))
        def _():
            out_ring.hop_piece(d + 1, 0)

        @pl.when(d >= 2)
        def _():
            dense((kv_ring.owner(0, d - 1), kv_ring.owner(1, d - 1)))

        @pl.when((d + 1 < half))
        def _():
            out_ring.hop_piece(d + 1, 1)

        @pl.when((d + 1 == half))
        def _():
            out_ring.last()

        @pl.when(d == 3)
        def _():
            for c in halos:
                c.wait_recv()

        @pl.when((d >= 3) & (d < 3 + length // 128))
        def _():
            window(d - 3)

        return carry

    for p in range(2):
        out_ring.hop_piece(1, p)
    lax.fori_loop(1, half + 1, kv_step, 0)
    kv_ring.last()
    dense((me, kv_ring.owner(0, half)))
    both = jnp.concatenate(
        [a_s[:HD, h * length : h * length + length] / a_s[HD : HD + 1, h * length : h * length + length] for h in range(2)],
        axis=0,
    )
    for rows in blocks:
        attw[1, rows] = both[:, rows].T.astype(BF16)
    for t in range(n_tp):
        at = (t % 2) * half_rows + (t // 2) * share
        for which in range(2):
            att[at : at + share, which * 128 : which * 128 + 128] = attw[
                which, t * share : t * share + share
            ]

    def owners_of(s):
        return (
            lax.rem(me + n_sp - lax.rem(s, half), n_sp),
            lax.rem(me + s, n_sp),
        )

    theirs_at = pl.multiple_of((1 - core) * half_rows, half_rows)
    mine_at = pl.multiple_of(core * half_rows, half_rows)
    up = lax.rem(xc + 1, n_x)
    down = lax.rem(xc + n_x - 1, n_x)
    far = lax.rem(xc + 2, n_x)
    ways = ((x_up, up, x_down, down), (x_down, down, x_up, up))

    def pair_copy(s):
        return remote(dsend.at[s], drecv.at[s], d_s.at[lax.rem(s, 2)], d_r.at[s], partner)

    def far_copy(s, b):
        return remote(xs.at[s, b, far], r2.at[s, b], x_s.at[0, lax.rem(s, 4), b], x_r.at[0, s, b], ways[b][0])

    def chain_copy(s, b):
        return remote(c1.at[s, b], rc.at[s, b], x_s.at[1, lax.rem(s, 4), b], x_r.at[1, s, b], ways[b][0])

    def near_copy(s, b):
        return remote(
            xs.at[s, b, ways[b][3]], rd.at[s, b], x_s.at[2, lax.rem(s, 4), b], x_r.at[2, s, b], ways[b][2]
        )

    def put(s, b):
        at = pl.multiple_of(owners_of(s)[b] * cols, cols)
        return pltpu.make_async_copy(held.at[s - 1, b], out.at[:, pl.ds(at, cols)], o_s.at[lax.rem(s, 2), b])

    def stage1(s):
        owners = owners_of(s)
        for b in range(2):
            dsend[s - 1, b] = nn(att[pl.ds(theirs_at, half_rows)], oall[owners[b]]).astype(BF16)
        mine[s - 1, 0] = nn(att[pl.ds(mine_at, half_rows)], oall[owners[0]])

        @pl.when(s > 2)
        def _():
            pair_copy(s - 3).wait_send()

        pair_copy(s - 1).start()
        mine[s - 1, 1] = nn(att[pl.ds(mine_at, half_rows)], oall[owners[1]])

    def stage2(s):
        pair_copy(s - 1).wait_recv()
        for b in range(2):
            both = (mine[s - 1, b] + drecv[s - 1, b].astype(F32)).astype(BF16)
            for t in range(n_x):
                xs[s - 1, b, t] = both[t * share : t * share + share]

        @pl.when(s > 4)
        def _():
            for b in range(2):
                far_copy(s - 5, b).wait_send()

        for b in range(2):
            far_copy(s - 1, b).start()

    def stage3(s):
        for b in range(2):
            far_copy(s - 1, b).wait_recv()
            c1[s - 1, b] = (xs[s - 1, b, ways[b][1]].astype(F32) + r2[s - 1, b].astype(F32)).astype(
                BF16
            )

        @pl.when(s > 4)
        def _():
            for b in range(2):
                chain_copy(s - 5, b).wait_send()

        for b in range(2):
            chain_copy(s - 1, b).start()

    def send_near(s):
        @pl.when(s > 4)
        def _():
            for b in range(2):
                near_copy(s - 5, b).wait_send()

        for b in range(2):
            near_copy(s - 1, b).start()

    def stage4(s):
        for b in range(2):
            chain_copy(s - 1, b).wait_recv()
            near_copy(s - 1, b).wait_recv()
            total = (
                xs[s - 1, b, xc].astype(F32) + rc[s - 1, b].astype(F32) + rd[s - 1, b].astype(F32)
            )
            held[s - 1, b] = total.astype(BF16)

        @pl.when(s > 2)
        def _():
            for b in range(2):
                put(s - 2, b).wait()

        for b in range(2):
            put(s, b).start()

    def out_step(s, carry):
        @pl.when(s < half)
        def _():
            out_ring.take(s)

        @pl.when(s == half)
        def _():
            out_ring.take_last()

        @pl.when(s <= half)
        def _():
            stage1(s)

        @pl.when((s >= 1 + LAG[0]) & (s <= half + LAG[0]))
        def _():
            stage2(s - LAG[0])

        @pl.when((s >= 1 + LAG[1]) & (s <= half + LAG[1]))
        def _():
            stage3(s - LAG[1])

        @pl.when((s >= 1 + LAG[2]) & (s <= half + LAG[2]))
        def _():
            send_near(s - LAG[2])

        @pl.when(s >= 1 + LAG[3])
        def _():
            stage4(s - LAG[3])

        @pl.when(s == 3)
        def _():
            in_ring.drain()
            kv_ring.drain()
            for c in halos:
                c.wait_send()

        return carry

    lax.fori_loop(1, half + LAG[3] + 1, out_step, 0)

    out_ring.drain()

    def drain(s, carry):
        for b in range(2):
            far_copy(s, b).wait_send()
            near_copy(s, b).wait_send()
            chain_copy(s, b).wait_send()
        return carry

    lax.fori_loop(half - 4, half, drain, 0)
    for s in (half - 2, half - 1):
        pair_copy(s).wait_send()
        for b in range(2):
            put(s + 1, b).wait()


def frequencies():
    lane = np.arange(128)
    line = THETA ** (-2.0 * (lane % (HD // 2)) / HD)
    grid = THETA ** (-2.0 * (lane % (HD // 4)) / (HD // 2))
    return np.stack([line, grid]).astype(np.float32)


def solution(mesh):
    n_sp, n_tp = mesh.shape["sp"], mesh.shape["tp"]
    assert n_sp % 2 == 0 and n_tp == 8 and mesh.shape["grp"] % 2 == 0

    def local(tokens, gain, wq, wk, wv, wqg, wkg, sink, dq, dk, dv, dqg, dkg, wo, do):
        length, width = tokens.shape
        depth, cols = wq.shape[0], wo.shape[1]
        half, n_x, share = n_sp // 2, n_tp // 2, length // n_tp
        assert wq.shape[1] == dq.shape[1] == 2 * HD and wk.shape[1] == dk.shape[1] == HD
        assert length % 128 == 0 and share % 16 == 0 and width == depth * n_sp
        any_ = pl.BlockSpec(memory_space=pl.ANY)
        smem = pl.BlockSpec(memory_space=pltpu.SMEM)
        dma = pltpu.SemaphoreType.DMA
        return pl.pallas_call(
            functools.partial(kernel, n_sp, n_tp),
            out_shape=jax.ShapeDtypeStruct((share, cols * n_sp), BF16),
            in_specs=[any_] * 7 + [smem] + [any_] * 8,
            out_specs=any_,
            scratch_shapes=[
                pltpu.VMEM((length, width), BF16),
                pltpu.VMEM((n_sp, depth, 512), BF16),
                pltpu.VMEM((4, HD, depth), BF16),
                pltpu.VMEM((length, 512), F32),
                pltpu.VMEM((n_sp, 256, cols), BF16),
                pltpu.VMEM((n_sp, length // 2, 128), BF16),
                pltpu.VMEM((n_sp, HD, length), BF16),
                pltpu.VMEM((length + 2 * WINDOW, 128), BF16),
                pltpu.VMEM((2, 128, 2 * length), BF16),
                pltpu.VMEM((2, length, 128), BF16),
                pltpu.VMEM((length, 256), BF16),
                pltpu.VMEM((2, length, 128), BF16),
                pltpu.VMEM((8, 2 * length), F32),
                pltpu.VMEM((HD + 8, 2 * length), F32),
                pltpu.VMEM((4, length, 128), F32),
                pltpu.VMEM((half, 2, length // 2, cols), BF16),
                pltpu.VMEM((half, 2, length // 2, cols), BF16),
                pltpu.VMEM((half, 2, length // 2, cols), F32),
                pltpu.VMEM((half, 2, n_x, share, cols), BF16),
                pltpu.VMEM((half, 2, share, cols), BF16),
                pltpu.VMEM((half, 2, share, cols), BF16),
                pltpu.VMEM((half, 2, share, cols), BF16),
                pltpu.VMEM((half, 2, share, cols), BF16),
                dma((18,)),
                dma((2, 2, 4)),
                dma((2, half, 4)),
                dma((2, 2, 2)),
                dma((2,)),
                dma((2,)),
                dma((2,)),
                dma((half,)),
                dma((3, 4, 2)),
                dma((3, half, 2)),
                dma((2, 2)),
                dma((2, half)),
                dma((2, 2)),
                dma((2, half)),
                pltpu.VMEM((half, 2, share, cols), BF16),
                dma((2, 2)),
                pltpu.VMEM((width // 128, 128), F32),
                pltpu.VMEM((4, 1, HD), F32),
                pltpu.VMEM((2, 128), F32),
                dma((2, 2, 2)),
            ],
            compiler_params=pltpu.CompilerParams(
                collective_id=0, has_side_effects=True, vmem_limit_bytes=60 * 1024 * 1024
            ),
        )(
            tokens, gain.reshape(-1, 128), wq, wk.T, wv.T, wqg[None], wkg[None], sink,
            dq, dk.T, dv.T, dqg[None], dkg[None], wo, do, jnp.asarray(frequencies()),
        )

    return jax.shard_map(
        local,
        mesh=mesh,
        in_specs=(
            P(("grp", "sp"), None),
            P(),
            P("sp", "tp"),
            P("sp", "tp"),
            P("sp", "tp"),
            P(),
            P(),
            P("tp"),
            P("sp", "tp"),
            P("sp", "tp"),
            P("sp", "tp"),
            P(),
            P(),
            P("tp", "sp"),
            P("tp", "sp"),
        ),
        out_specs=P(("grp", "sp", "tp"), None),
        check_vma=False,
    )
```

```python
import functools
import math

import jax
import jax.numpy as jnp
import numpy as np
from jax import lax
from jax.experimental import pallas as pl
from jax.experimental.pallas import tpu as pltpu
from jax.sharding import PartitionSpec as P

HD = 64
WINDOW = 128
GRID_W = 64
EPS = 1e-06
THETA = 10000.0
MESH = pl.DeviceIdType.MESH
F32 = jnp.float32
BF16 = jnp.bfloat16
LOW = -1e30
LAG = (1, 5, 2, 13)
EARLY = 1


def nt(a, b):
    return lax.dot_general(a, b, (((1,), (1,)), ((), ())), preferred_element_type=F32)


def nn(a, b):
    return jnp.dot(a, b, preferred_element_type=F32)


def remote(src, dst, send, recv, device):
    return pltpu.make_async_remote_copy(
        src_ref=src, dst_ref=dst, send_sem=send, recv_sem=recv, device_id=device, device_id_type=MESH
    )


class Ring:
    def __init__(self, me, n, count, piece, send_sem, recv_sem):
        self.me, self.n, self.half = me, n, n // 2
        self.count = count
        self.piece, self.send_sem, self.recv_sem = piece, send_sem, recv_sem
        self.to = ({"sp": lax.rem(me + 1, n)}, {"sp": lax.rem(me + n - 1, n)})

    def owner(self, way, step):
        shift = self.n - step if way == 0 else step
        return lax.rem(self.me + shift, self.n)

    def copy(self, way, step, p, distance):
        ref = self.piece(self.owner(way, distance), p)
        return remote(
            ref, ref, self.send_sem.at[way, lax.rem(step, 2), p], self.recv_sem.at[way, step, p], self.to[way]
        )

    def send(self, way, step, p):
        @pl.when(step >= 2)
        def _():
            self.copy(way, step - 2, p, step - 2).wait_send()

        self.copy(way, step, p, step).start()

    def wait(self, way, step, p):
        self.copy(way, step, p, step + 1).wait_recv()

    def way_of(self, p):
        return 2 * p // self.count

    def begin(self, pieces=None):
        for p in pieces or range(self.count):
            for way in range(2):
                self.copy(way, 0, p, 0).start()

    def hop_piece(self, step, p):
        for way in range(2):
            self.wait(way, step - 1, p)

            @pl.when((step < self.half - 1) | (self.way_of(p) == way))
            def _():
                self.send(way, step, p)

    def wait_last(self, way):
        for p in range(self.count):
            if self.way_of(p) == way:
                self.wait(way, self.half - 1, p)

    def last(self):
        for way in range(2):
            self.wait_last(way)

    def drain(self):
        for way in range(2):
            for p in range(self.count):
                final = self.half - 1 if self.way_of(p) == way else self.half - 2
                for step in (final - 1, final):
                    self.copy(way, step, p, step).wait_send()


class PairRing(Ring):
    def __init__(self, me, n, ref, give, side, other, send_sem, recv_sem, pair_send, pair_recv):
        rows = ref.shape[1]
        common = rows - 2 * give
        self.ref, self.give, self.other = ref, give, other
        self.given_at = pl.multiple_of(side * (rows - give), 16)
        self.taken_at = pl.multiple_of((1 - side) * (rows - give), 16)
        self.pair_send, self.pair_recv = pair_send, pair_recv
        if common:
            first = give // 32 * 16
            cuts = [(0, first), (first, give - first)]
            later = [(give, common // 2), (give + common // 2, common - common // 2)]
        else:
            cuts, later = [(0, give // 2), (give // 2, give // 2)], []
        self.cross_after = 1
        self.early_cross = bool(later)

        def piece(w, p):
            if p < 2:
                at = pl.multiple_of(self.given_at + cuts[p][0], 16)
                return ref.at[w, pl.ds(at, cuts[p][1])]
            return ref.at[w, pl.ds(*later[p - 2])]

        super().__init__(me, n, 2 + len(later), piece, send_sem, recv_sem)

    def across(self, way, step, at):
        ref = self.ref.at[self.owner(way, step), pl.ds(at, self.give)]
        return remote(
            ref, ref, self.pair_send.at[way, lax.rem(step, 2)], self.pair_recv.at[way, step - 1], self.other
        )

    def hop_piece(self, step, p):
        super().hop_piece(step, p)
        if p == self.cross_after:
            for way in range(2):

                @pl.when(step >= 3)
                def _():
                    self.across(way, step - 2, self.given_at).wait_send()

                self.across(way, step, self.given_at).start()

    def last_first(self):
        self.wait_last(0)
        if not self.early_cross:
            self.wait_last(1)
        self.across(0, self.half - 2, self.given_at).wait_send()
        self.across(0, self.half, self.given_at).start()

    def last_second(self):
        if self.early_cross:
            self.wait_last(1)

    def last(self):
        self.last_first()
        self.last_second()

    def take(self, step):
        for way in range(2):
            self.across(way, step, self.taken_at).wait_recv()

    def take_last(self):
        self.across(0, self.half, self.taken_at).wait_recv()

    def drain_pair(self):
        self.across(0, self.half, self.given_at).wait_send()
        for way in range(2):
            self.across(way, self.half - 1, self.given_at).wait_send()
        self.across(1, self.half - 2, self.given_at).wait_send()


def kernel(
    n_sp, n_tp,
    tokens, gain_h, wq, wk, wv, wqg_h, wkg_h, sink, dq, dk, dv, dqg_h, dkg_h, wo, do, freq_h,
    out,
    x, wall, stage, acc, oall, kp, vt, kvw, qd, qw, att, attw, m_s, a_s,
    table, dsend, drecv, mine, xs, r2, c1, rc, rd,
    in_s, in_r, out_s, out_r, halo_s, halo_r,
    d_s, d_r, x_r, in_ys, in_yr, out_ys, out_yr, held, o_s,
    gain, gains, freq, kv_snd,
):
    me = lax.axis_index("sp")
    tp = lax.axis_index("tp")
    core = lax.rem(tp, 2)
    xc = lax.div(tp, 2)
    n_x = n_tp // 2
    length, width = x.shape
    depth = wall.shape[1]
    cols = oall.shape[2]
    half_rows = length // 2
    share = length // n_tp
    half = n_sp // 2
    right, left = {"sp": lax.rem(me + 1, n_sp)}, {"sp": lax.rem(me + n_sp - 1, n_sp)}
    partner = {"tp": xc * 2 + (1 - core)}
    x_up = {"tp": lax.rem(xc + 1, n_x) * 2 + core}
    x_down = {"tp": lax.rem(xc + n_x - 1, n_x) * 2 + core}

    grp = lax.axis_index("grp")
    side = lax.rem(grp, 2)
    other = {"grp": grp + 1 - 2 * side}

    barrier = pltpu.get_barrier_semaphore()
    for peer in (right, left, partner, x_up, x_down, other):
        pl.semaphore_signal(barrier, inc=1, device_id=peer, device_id_type=MESH)

    load_sems = [kv_snd.at[i // 8, i // 4 % 2, i % 4] for i in range(16)]
    load_sems += [halo_s.at[i] for i in range(2)]
    loads = [
        pltpu.make_async_copy(wk, stage.at[0], load_sems[0]),
        pltpu.make_async_copy(wv, stage.at[1], load_sems[1]),
        pltpu.make_async_copy(dk, stage.at[2], load_sems[2]),
        pltpu.make_async_copy(dv, stage.at[3], load_sems[3]),
        pltpu.make_async_copy(wq, wall.at[me, :, pl.ds(0, 128)], load_sems[4]),
        pltpu.make_async_copy(dq, wall.at[me, :, pl.ds(256, 128)], load_sems[5]),
        pltpu.make_async_copy(wo, oall.at[me, pl.ds(0, 128)], load_sems[6]),
        pltpu.make_async_copy(do, oall.at[me, pl.ds(128, 128)], load_sems[7]),
    ]
    small = [
        pltpu.make_async_copy(src, dst, load_sems[12 + i])
        for i, (src, dst) in enumerate(
            [(gain_h, gain), (freq_h, freq)]
            + [(g, gains.at[j]) for j, g in enumerate((wqg_h, wkg_h, dqg_h, dkg_h))]
        )
    ]
    for c in loads:
        c.start()
    quarter = length // 4
    token_loads = [
        pltpu.make_async_copy(
            tokens.at[pl.ds(i * quarter, quarter)], x.at[pl.ds(i * quarter, quarter)], load_sems[8 + i]
        )
        for i in range(4)
    ]
    for c in token_loads + small:
        c.start()
    for c in loads[:4]:
        c.wait()
    for at, base in ((0, 128), (2, 384)):
        pair = jnp.concatenate([stage[at], stage[at + 1]], axis=0).astype(F32)
        wall[me, :, base : base + 128] = pair.T.astype(BF16)
    for c in loads[4:]:
        c.wait()
    pl.semaphore_wait(barrier, 6)

    pair_rows = (kp.shape[1] // 2, vt.shape[1] // 2)
    in_ring = PairRing(me, n_sp, wall, depth * 5 // 16, side, other, in_s, in_r, in_ys, in_yr)
    out_ring = PairRing(me, n_sp, oall, 128, side, other, out_s, out_r, out_ys, out_yr)
    kv_ring = Ring(
        me, n_sp, 4,
        lambda w, p: (kp, vt)[p // 2].at[w, pl.ds(p % 2 * (pair_rows[p // 2]), pair_rows[p // 2])],
        kv_snd, in_r,
    )
    in_ring.begin()
    for c in small:
        c.wait()

    def norm(i):
        token_loads[i].wait()

        def norm_rows(r, carry):
            at = pl.multiple_of(i * quarter + r * 16, 16)
            total = jnp.zeros((16, 128), F32)
            for j in range(width // 128):
                piece = x[pl.ds(at, 16), j * 128 : j * 128 + 128].astype(F32)
                total = total + piece * piece
            scale = lax.rsqrt(jnp.sum(total, axis=-1, keepdims=True) * (1.0 / width) + EPS)
            for j in range(width // 128):
                piece = x[pl.ds(at, 16), j * 128 : j * 128 + 128].astype(F32)
                x[pl.ds(at, 16), j * 128 : j * 128 + 128] = (
                    piece * scale * gain[j : j + 1, :]
                ).astype(BF16)
            return carry

        lax.fori_loop(0, quarter // 16, norm_rows, 0)

    lane = lax.broadcasted_iota(jnp.int32, (1, 128), 1)
    low_lane = lane < HD

    def tables(r, carry):
        at = pl.multiple_of(r * 64, 64)
        place = me * length + at + lax.broadcasted_iota(jnp.int32, (64, 128), 0)
        angle = place.astype(F32) * freq[0:1, :]
        table[0, pl.ds(at, 64)] = jnp.cos(angle)
        table[1, pl.ds(at, 64)] = jnp.sin(angle)
        row = lax.div(place, GRID_W)
        spot = jnp.where(lax.rem(lane, HD) < HD // 2, row, place - row * GRID_W)
        angle = spot.astype(F32) * freq[1:2, :]
        table[2, pl.ds(at, 64)] = jnp.cos(angle)
        table[3, pl.ds(at, 64)] = jnp.sin(angle)
        return carry

    def project(w, first=False):
        at = pl.multiple_of(w * depth, depth)
        product = nn(x[:, pl.ds(at, depth)], wall[w])
        if first:
            acc[...] = product
        else:
            acc[...] += product

    def projects(d, carry):
        in_ring.take(d)
        project(in_ring.owner(0, d))
        project(in_ring.owner(1, d))
        return carry

    def in_step(d, carry):
        in_ring.hop_piece(d, 0)
        in_ring.hop_piece(d, 1)

        @pl.when(d == 1)
        def _():
            norm(0)
            norm(1)

        @pl.when(d == 2)
        def _():
            norm(2)
            norm(3)

        @pl.when(d == 3)
        def _():
            lax.fori_loop(0, length // 64, tables, 0)
            project(me, first=True)

        @pl.when(d >= 4)
        def _():
            lax.fori_loop(jnp.where(d == 4, 1, d - 2), d - 1, projects, 0)

        in_ring.hop_piece(d, 2)
        in_ring.hop_piece(d, 3)
        return carry

    lax.fori_loop(1, half, in_step, 0)
    out_ring.begin()
    projects(half - 2, 0)
    in_ring.last_first()
    projects(half - 1, 0)
    in_ring.last_second()
    for p in range(2):
        out_ring.hop_piece(1, p)
    in_ring.take_last()
    project(in_ring.owner(0, half))

    def two(which):
        return jnp.concatenate([gains[which], gains[which]], axis=1)

    def heads(values, g, which, reach, rows):
        squares = values * values
        low = jnp.sum(jnp.where(low_lane, squares, 0.0), axis=-1, keepdims=True)
        high = jnp.sum(jnp.where(low_lane, 0.0, squares), axis=-1, keepdims=True)
        mean = jnp.where(low_lane, low, high) * (1.0 / HD)
        normed = values * lax.rsqrt(mean + EPS) * g
        turned = jnp.where(
            lax.rem(lane, 2 * reach) < reach,
            -pltpu.roll(normed, 128 - reach, 1),
            pltpu.roll(normed, reach, 1),
        )
        return normed * table[which, rows] + turned * table[which + 1, rows]

    blocks = [slice(i * 128, i * 128 + 128) for i in range(length // 128)]
    g = two(3)
    keys = [
        heads(acc[rows, 384:512], g, 2, HD // 4, rows)
        for rows in (slice(0, half_rows), slice(half_rows, length))
    ]
    kp[me] = jnp.where(low_lane, keys[0], pltpu.roll(keys[1], HD, 1)).astype(BF16)
    for rows in blocks:
        vt[me, :, rows] = acc[rows, 384:512].T[HD:].astype(BF16)
    kv_ring.begin((0, 1))
    g = two(1)
    for i, rows in enumerate(blocks):
        values = acc[rows, 128:256]
        kvw[pl.ds(WINDOW + i * 128, 128)] = jnp.where(
            low_lane, heads(values, g, 0, HD // 2, rows), values
        ).astype(BF16)
    kv_ring.begin((2, 3))
    halos = [
        remote(
            kvw.at[pl.ds(length, WINDOW)], kvw.at[pl.ds(0, WINDOW)], halo_s.at[0], halo_r.at[0], right
        ),
        remote(
            kvw.at[pl.ds(WINDOW, WINDOW)],
            kvw.at[pl.ds(WINDOW + length, WINDOW)],
            halo_s.at[1],
            halo_r.at[1],
            left,
        ),
    ]
    for c in halos:
        c.start()
    scale = HD ** (-0.5)
    g = two(2)
    for rows in blocks:
        q = heads(acc[rows, 256:384], g, 2, HD // 4, rows) * (scale * math.log2(math.e))
        q = q.T.astype(BF16)
        for h in range(2):
            for p in range(2):
                cols_h = slice(h * length + rows.start, h * length + rows.stop)
                qd[p, p * HD : p * HD + HD, cols_h] = q[h * HD : h * HD + HD]
                qd[p, (1 - p) * HD : (1 - p) * HD + HD, cols_h] = jnp.zeros((HD, 128), BF16)
    g = two(0)
    for rows in blocks:
        q = heads(acc[rows, 0:128], g, 0, HD // 2, rows).astype(BF16).astype(F32) * scale
        qw[0, rows] = jnp.where(low_lane, q, 0.0).astype(BF16)
        qw[1, rows] = jnp.where(low_lane, pltpu.roll(q, HD, 1), 0.0).astype(BF16)

    m_s[...] = jnp.full(m_s.shape, LOW, F32)
    a_s[...] = jnp.zeros(a_s.shape, F32)

    def window(i):
        at = pl.multiple_of(i * 128, 128)
        queries = jnp.concatenate([qw[0, pl.ds(at, 128)], qw[1, pl.ds(at, 128)]], axis=0)
        near = kvw[pl.ds(at, 3 * WINDOW)]
        scores = nt(queries, near)
        row = lax.broadcasted_iota(jnp.int32, scores.shape, 0)
        key = lax.broadcasted_iota(jnp.int32, scores.shape, 1)
        first = row < 128
        spot = jnp.where(first, row, row - 128)
        place = me * length + at - WINDOW + key
        valid = (
            (key >= spot)
            & (key <= spot + 2 * WINDOW)
            & (place >= 0)
            & (place < length * n_sp)
        )
        scores = jnp.where(valid, scores, LOW)
        floor = jnp.where(
            lax.broadcasted_iota(jnp.int32, (256, 1), 0) < 128, sink[0], sink[1]
        )
        top = jnp.maximum(jnp.max(scores, axis=-1, keepdims=True), floor)
        expon = jnp.exp(scores - top)
        total = jnp.sum(expon, axis=-1, keepdims=True) + jnp.exp(floor - top)
        weights = (expon / total).astype(BF16)
        result = nn(weights, near)
        attw[0, pl.ds(at, 128)] = jnp.where(
            low_lane, pltpu.roll(result[:128], HD, 1), result[128:]
        ).astype(BF16)

    ones = jnp.ones((8, 2 * length), BF16)

    def dense(owners, cut=slice(None)):
        keys = jnp.concatenate([kp[w] for w in owners], axis=0)
        values = jnp.concatenate(
            [jnp.concatenate([vt[w] for w in owners], axis=1), ones], axis=0
        )
        low, high = nn(keys, qd[0, :, cut]), nn(keys, qd[1, :, cut])
        before = m_s[:, cut]
        top = jnp.maximum(before, jnp.max(jnp.maximum(low, high), axis=0, keepdims=True))
        shrink = jnp.exp2(before - top)
        low = jnp.exp2(low - top[:1]).astype(BF16)
        high = jnp.exp2(high - top[:1]).astype(BF16)
        expons = jnp.concatenate(
            [low[:half_rows], high[:half_rows], low[half_rows:], high[half_rows:]], axis=0
        )
        a_s[:, cut] = a_s[:, cut] * shrink[:1] + nn(values, expons)
        m_s[:, cut] = top

    def kv_step(d, carry):
        for h in range(2):

            @pl.when(d < half)
            def _():
                kv_ring.hop_piece(d, 2 * h)
                kv_ring.hop_piece(d, 2 * h + 1)

            @pl.when(d >= 2)
            def _():
                dense(
                    (kv_ring.owner(0, d - 1), kv_ring.owner(1, d - 1)),
                    slice(h * length, h * length + length),
                )

        @pl.when(d + EARLY < half)
        def _():
            out_ring.hop_piece(d + EARLY, 0)

        @pl.when((d >= 3) & (d < 3 + length // 128))
        def _():
            window(d - 3)

        @pl.when(d + EARLY < half)
        def _():
            out_ring.hop_piece(d + EARLY, 1)

        @pl.when(d + EARLY == half)
        def _():
            out_ring.last()

        @pl.when(d == 2)
        def _():
            for c in halos:
                c.wait_recv()

        return carry

    for h in range(2, EARLY + 1):
        for p in range(2):
            out_ring.hop_piece(h, p)
    lax.fori_loop(1, half + 1, kv_step, 0)
    kv_ring.last()
    dense((me, kv_ring.owner(0, half)))
    both = jnp.concatenate(
        [a_s[:HD, h * length : h * length + length] / a_s[HD : HD + 1, h * length : h * length + length] for h in range(2)],
        axis=0,
    )
    for rows in blocks:
        attw[1, rows] = both[:, rows].T.astype(BF16)
    for t in range(n_tp):
        at = (t % 2) * half_rows + (t // 2) * share
        for which in range(2):
            att[at : at + share, which * 128 : which * 128 + 128] = attw[
                which, t * share : t * share + share
            ]

    def owners_of(s):
        return (
            lax.rem(me + n_sp - lax.rem(s, half), n_sp),
            lax.rem(me + s, n_sp),
        )

    theirs_at = pl.multiple_of((1 - core) * half_rows, half_rows)
    mine_at = pl.multiple_of(core * half_rows, half_rows)
    up = lax.rem(xc + 1, n_x)
    down = lax.rem(xc + n_x - 1, n_x)
    far = lax.rem(xc + 2, n_x)
    ways = ((x_up, up, x_down, down), (x_down, down, x_up, up))

    def pair_copy(s):
        return remote(dsend.at[s], drecv.at[s], d_s.at[lax.rem(s, 2)], d_r.at[s], partner)

    def far_copy(s, b):
        return remote(xs.at[s, b, far], r2.at[s, b], in_s.at[0, b, lax.rem(s, 4)], x_r.at[0, s, b], ways[b][0])

    def chain_copy(s, b):
        return remote(c1.at[s, b], rc.at[s, b], in_s.at[1, b, lax.rem(s, 4)], x_r.at[1, s, b], ways[b][0])

    def near_copy(s, b):
        return remote(
            xs.at[s, b, ways[b][3]], rd.at[s, b], out_s.at[b, lax.div(lax.rem(s, 4), 2), lax.rem(s, 2)], x_r.at[2, s, b], ways[b][2]
        )

    def put(s, b):
        at = pl.multiple_of(owners_of(s)[b] * cols, cols)
        return pltpu.make_async_copy(held.at[s - 1, b], out.at[:, pl.ds(at, cols)], o_s.at[lax.rem(s, 2), b])

    def stage1(s):
        owners = owners_of(s)
        for b in range(2):
            dsend[s - 1, b] = nn(att[pl.ds(theirs_at, half_rows)], oall[owners[b]]).astype(BF16)
        mine[s - 1, 0] = nn(att[pl.ds(mine_at, half_rows)], oall[owners[0]])

        @pl.when(s > 2)
        def _():
            pair_copy(s - 3).wait_send()

        pair_copy(s - 1).start()
        mine[s - 1, 1] = nn(att[pl.ds(mine_at, half_rows)], oall[owners[1]])

    def stage2(s):
        pair_copy(s - 1).wait_recv()
        for b in range(2):
            both = (mine[s - 1, b] + drecv[s - 1, b].astype(F32)).astype(BF16)
            for t in range(n_x):
                xs[s - 1, b, t] = both[t * share : t * share + share]

        @pl.when(s > 4)
        def _():
            for b in range(2):
                far_copy(s - 5, b).wait_send()

        for b in range(2):
            far_copy(s - 1, b).start()

    def stage3(s):
        for b in range(2):
            far_copy(s - 1, b).wait_recv()
            c1[s - 1, b] = (xs[s - 1, b, ways[b][1]].astype(F32) + r2[s - 1, b].astype(F32)).astype(
                BF16
            )

        @pl.when(s > 4)
        def _():
            for b in range(2):
                chain_copy(s - 5, b).wait_send()

        for b in range(2):
            chain_copy(s - 1, b).start()

    def send_near(s):
        @pl.when(s > 4)
        def _():
            for b in range(2):
                near_copy(s - 5, b).wait_send()

        for b in range(2):
            near_copy(s - 1, b).start()

    def stage4(s):
        for b in range(2):
            chain_copy(s - 1, b).wait_recv()
            near_copy(s - 1, b).wait_recv()
            total = (
                xs[s - 1, b, xc].astype(F32) + rc[s - 1, b].astype(F32) + rd[s - 1, b].astype(F32)
            )
            held[s - 1, b] = total.astype(BF16)

        @pl.when(s > 2)
        def _():
            for b in range(2):
                put(s - 2, b).wait()

        for b in range(2):
            put(s, b).start()

    def out_step(s, carry):
        @pl.when(s < half)
        def _():
            out_ring.take(s)

        @pl.when(s == half)
        def _():
            out_ring.take_last()

        @pl.when(s <= half)
        def _():
            stage1(s)

        @pl.when((s >= 1 + LAG[0]) & (s <= half + LAG[0]))
        def _():
            stage2(s - LAG[0])

        @pl.when((s >= 1 + LAG[1]) & (s <= half + LAG[1]))
        def _():
            stage3(s - LAG[1])

        @pl.when((s >= 1 + LAG[2]) & (s <= half + LAG[2]))
        def _():
            send_near(s - LAG[2])

        @pl.when(s >= 1 + LAG[3])
        def _():
            stage4(s - LAG[3])

        @pl.when(s == 3)
        def _():
            in_ring.drain_pair()
            kv_ring.drain()
            for c in halos:
                c.wait_send()

        return carry

    in_ring.drain()
    out_ring.drain()
    lax.fori_loop(1, half + LAG[3] + 1, out_step, 0)

    out_ring.drain_pair()

    def drain(s, carry):
        for b in range(2):
            far_copy(s, b).wait_send()
            near_copy(s, b).wait_send()
            chain_copy(s, b).wait_send()
        return carry

    lax.fori_loop(half - 4, half, drain, 0)
    for s in (half - 2, half - 1):
        pair_copy(s).wait_send()
        for b in range(2):
            put(s + 1, b).wait()


def frequencies():
    lane = np.arange(128)
    line = THETA ** (-2.0 * (lane % (HD // 2)) / HD)
    grid = THETA ** (-2.0 * (lane % (HD // 4)) / (HD // 2))
    return np.stack([line, grid]).astype(np.float32)


def solution(mesh):
    n_sp, n_tp = mesh.shape["sp"], mesh.shape["tp"]
    assert n_sp % 2 == 0 and n_tp == 8 and mesh.shape["grp"] % 2 == 0

    def local(tokens, gain, wq, wk, wv, wqg, wkg, sink, dq, dk, dv, dqg, dkg, wo, do):
        length, width = tokens.shape
        depth, cols = wq.shape[0], wo.shape[1]
        half, n_x, share = n_sp // 2, n_tp // 2, length // n_tp
        assert wq.shape[1] == dq.shape[1] == 2 * HD and wk.shape[1] == dk.shape[1] == HD
        assert length % 128 == 0 and share % 16 == 0 and width == depth * n_sp
        any_ = pl.BlockSpec(memory_space=pl.ANY)
        smem = pl.BlockSpec(memory_space=pltpu.SMEM)
        dma = pltpu.SemaphoreType.DMA
        return pl.pallas_call(
            functools.partial(kernel, n_sp, n_tp),
            out_shape=jax.ShapeDtypeStruct((share, cols * n_sp), BF16),
            in_specs=[any_] * 7 + [smem] + [any_] * 8,
            out_specs=any_,
            scratch_shapes=[
                pltpu.VMEM((length, width), BF16),
                pltpu.VMEM((n_sp, depth, 512), BF16),
                pltpu.VMEM((4, HD, depth), BF16),
                pltpu.VMEM((length, 512), F32),
                pltpu.VMEM((n_sp, 256, cols), BF16),
                pltpu.VMEM((n_sp, length // 2, 128), BF16),
                pltpu.VMEM((n_sp, HD, length), BF16),
                pltpu.VMEM((length + 2 * WINDOW, 128), BF16),
                pltpu.VMEM((2, 128, 2 * length), BF16),
                pltpu.VMEM((2, length, 128), BF16),
                pltpu.VMEM((length, 256), BF16),
                pltpu.VMEM((2, length, 128), BF16),
                pltpu.VMEM((8, 2 * length), F32),
                pltpu.VMEM((HD + 8, 2 * length), F32),
                pltpu.VMEM((4, length, 128), F32),
                pltpu.VMEM((half, 2, length // 2, cols), BF16),
                pltpu.VMEM((half, 2, length // 2, cols), BF16),
                pltpu.VMEM((half, 2, length // 2, cols), F32),
                pltpu.VMEM((half, 2, n_x, share, cols), BF16),
                pltpu.VMEM((half, 2, share, cols), BF16),
                pltpu.VMEM((half, 2, share, cols), BF16),
                pltpu.VMEM((half, 2, share, cols), BF16),
                pltpu.VMEM((half, 2, share, cols), BF16),
                dma((2, 2, 4)),
                dma((2, half, 4)),
                dma((2, 2, 2)),
                dma((2, half, 2)),
                dma((2,)),
                dma((2,)),
                dma((2,)),
                dma((half,)),
                dma((3, half, 2)),
                dma((2, 2)),
                dma((2, half)),
                dma((2, 2)),
                dma((2, half)),
                pltpu.VMEM((half, 2, share, cols), BF16),
                dma((2, 2)),
                pltpu.VMEM((width // 128, 128), F32),
                pltpu.VMEM((4, 1, HD), F32),
                pltpu.VMEM((2, 128), F32),
                dma((2, 2, 4)),
            ],
            compiler_params=pltpu.CompilerParams(
                collective_id=0, has_side_effects=True, vmem_limit_bytes=60 * 1024 * 1024
            ),
        )(
            tokens, gain.reshape(-1, 128), wq, wk.T, wv.T, wqg[None], wkg[None], sink,
            dq, dk.T, dv.T, dqg[None], dkg[None], wo, do, jnp.asarray(frequencies()),
        )

    return jax.shard_map(
        local,
        mesh=mesh,
        in_specs=(
            P(("grp", "sp"), None),
            P(),
            P("sp", "tp"),
            P("sp", "tp"),
            P("sp", "tp"),
            P(),
            P(),
            P("tp"),
            P("sp", "tp"),
            P("sp", "tp"),
            P("sp", "tp"),
            P(),
            P(),
            P("tp", "sp"),
            P("tp", "sp"),
        ),
        out_specs=P(("grp", "sp", "tp"), None),
        check_vma=False,
    )
```

```python
import functools
import math

import jax
import jax.numpy as jnp
import numpy as np
from jax import lax
from jax.experimental import pallas as pl
from jax.experimental.pallas import tpu as pltpu
from jax.sharding import PartitionSpec as P

HD = 64
WINDOW = 128
GRID_W = 64
EPS = 1e-06
THETA = 10000.0
MESH = pl.DeviceIdType.MESH
F32 = jnp.float32
BF16 = jnp.bfloat16
LOW = -1e30
LAG = (1, 5, 2, 13)
EARLY = 1


def nt(a, b):
    return lax.dot_general(a, b, (((1,), (1,)), ((), ())), preferred_element_type=F32)


def nn(a, b):
    return jnp.dot(a, b, preferred_element_type=F32)


def remote(src, dst, send, recv, device):
    return pltpu.make_async_remote_copy(
        src_ref=src, dst_ref=dst, send_sem=send, recv_sem=recv, device_id=device, device_id_type=MESH
    )


class Ring:
    def __init__(self, me, n, count, piece, send_sem, recv_sem):
        self.me, self.n, self.half = me, n, n // 2
        self.count = count
        self.piece, self.send_sem, self.recv_sem = piece, send_sem, recv_sem
        self.to = ({"sp": lax.rem(me + 1, n)}, {"sp": lax.rem(me + n - 1, n)})

    def owner(self, way, step):
        shift = self.n - step if way == 0 else step
        return lax.rem(self.me + shift, self.n)

    def copy(self, way, step, p, distance):
        ref = self.piece(self.owner(way, distance), p)
        return remote(
            ref, ref, self.send_sem.at[way, lax.rem(step, 2), p], self.recv_sem.at[way, step, p], self.to[way]
        )

    def send(self, way, step, p):
        @pl.when(step >= 2)
        def _():
            self.copy(way, step - 2, p, step - 2).wait_send()

        self.copy(way, step, p, step).start()

    def wait(self, way, step, p):
        self.copy(way, step, p, step + 1).wait_recv()

    def way_of(self, p):
        return 2 * p // self.count

    def begin(self, pieces=None):
        for p in pieces or range(self.count):
            for way in range(2):
                self.copy(way, 0, p, 0).start()

    def hop_piece(self, step, p):
        for way in range(2):
            self.wait(way, step - 1, p)

            @pl.when((step < self.half - 1) | (self.way_of(p) == way))
            def _():
                self.send(way, step, p)

    def wait_last(self, way):
        for p in range(self.count):
            if self.way_of(p) == way:
                self.wait(way, self.half - 1, p)

    def last(self):
        for way in range(2):
            self.wait_last(way)

    def drain(self):
        for way in range(2):
            for p in range(self.count):
                final = self.half - 1 if self.way_of(p) == way else self.half - 2
                for step in (final - 1, final):
                    self.copy(way, step, p, step).wait_send()


class PairRing(Ring):
    def __init__(self, me, n, ref, give, side, other, send_sem, recv_sem, pair_send, pair_recv):
        rows = ref.shape[1]
        common = rows - 2 * give
        self.ref, self.give, self.other = ref, give, other
        self.given_at = pl.multiple_of(side * (rows - give), 16)
        self.taken_at = pl.multiple_of((1 - side) * (rows - give), 16)
        self.pair_send, self.pair_recv = pair_send, pair_recv
        if common:
            first = give // 32 * 16
            cuts = [(0, first), (first, give - first)]
            later = [(give, common // 2), (give + common // 2, common - common // 2)]
        else:
            cuts, later = [(0, give // 2), (give // 2, give // 2)], []
        self.cross_after = 1
        self.early_cross = bool(later)

        def piece(w, p):
            if p < 2:
                at = pl.multiple_of(self.given_at + cuts[p][0], 16)
                return ref.at[w, pl.ds(at, cuts[p][1])]
            return ref.at[w, pl.ds(*later[p - 2])]

        super().__init__(me, n, 2 + len(later), piece, send_sem, recv_sem)

    def across(self, way, step, at):
        ref = self.ref.at[self.owner(way, step), pl.ds(at, self.give)]
        return remote(
            ref, ref, self.pair_send.at[way, lax.rem(step, 2)], self.pair_recv.at[way, step - 1], self.other
        )

    def hop_piece(self, step, p):
        super().hop_piece(step, p)
        if p == self.cross_after:
            for way in range(2):

                @pl.when(step >= 3)
                def _():
                    self.across(way, step - 2, self.given_at).wait_send()

                self.across(way, step, self.given_at).start()

    def last_first(self):
        self.wait_last(0)
        if not self.early_cross:
            self.wait_last(1)
        self.across(0, self.half - 2, self.given_at).wait_send()
        self.across(0, self.half, self.given_at).start()

    def last_second(self):
        if self.early_cross:
            self.wait_last(1)

    def last(self):
        self.last_first()
        self.last_second()

    def take(self, step):
        for way in range(2):
            self.across(way, step, self.taken_at).wait_recv()

    def take_last(self):
        self.across(0, self.half, self.taken_at).wait_recv()

    def drain_pair(self):
        self.across(0, self.half, self.given_at).wait_send()
        for way in range(2):
            self.across(way, self.half - 1, self.given_at).wait_send()
        self.across(1, self.half - 2, self.given_at).wait_send()


def kernel(
    n_sp, n_tp,
    tokens, gain_h, wq, wk, wv, wqg_h, wkg_h, sink, dq, dk, dv, dqg_h, dkg_h, wo, do, freq_h,
    out,
    x, wall, stage, acc, oall, kp, vt, kvw, qd, qw, att, attw, m_s, a_s,
    table, dsend, drecv, mine, xs, r2, c1, rc, rd,
    in_s, in_r, out_s, out_r, halo_s, halo_r,
    d_s, d_r, x_r, in_ys, in_yr, out_ys, out_yr, gain, gains, freq, kv_snd,
):
    me = lax.axis_index("sp")
    tp = lax.axis_index("tp")
    core = lax.rem(tp, 2)
    xc = lax.div(tp, 2)
    n_x = n_tp // 2
    length, width = x.shape
    depth = wall.shape[1]
    cols = oall.shape[2]
    half_rows = length // 2
    share = length // n_tp
    half = n_sp // 2
    right, left = {"sp": lax.rem(me + 1, n_sp)}, {"sp": lax.rem(me + n_sp - 1, n_sp)}
    partner = {"tp": xc * 2 + (1 - core)}
    x_up = {"tp": lax.rem(xc + 1, n_x) * 2 + core}
    x_down = {"tp": lax.rem(xc + n_x - 1, n_x) * 2 + core}

    grp = lax.axis_index("grp")
    side = lax.rem(grp, 2)
    other = {"grp": grp + 1 - 2 * side}

    barrier = pltpu.get_barrier_semaphore()
    for peer in (right, left, partner, x_up, x_down, other):
        pl.semaphore_signal(barrier, inc=1, device_id=peer, device_id_type=MESH)

    load_sems = [kv_snd.at[i // 8, i // 4 % 2, i % 4] for i in range(16)]
    load_sems += [halo_s.at[i] for i in range(2)]
    loads = [
        pltpu.make_async_copy(wk, stage.at[0], load_sems[0]),
        pltpu.make_async_copy(wv, stage.at[1], load_sems[1]),
        pltpu.make_async_copy(dk, stage.at[2], load_sems[2]),
        pltpu.make_async_copy(dv, stage.at[3], load_sems[3]),
        pltpu.make_async_copy(wq, wall.at[me, :, pl.ds(0, 128)], load_sems[4]),
        pltpu.make_async_copy(dq, wall.at[me, :, pl.ds(256, 128)], load_sems[5]),
        pltpu.make_async_copy(wo, oall.at[me, pl.ds(0, 128)], load_sems[6]),
        pltpu.make_async_copy(do, oall.at[me, pl.ds(128, 128)], load_sems[7]),
    ]
    small = [
        pltpu.make_async_copy(src, dst, load_sems[12 + i])
        for i, (src, dst) in enumerate(
            [(gain_h, gain), (freq_h, freq)]
            + [(g, gains.at[j]) for j, g in enumerate((wqg_h, wkg_h, dqg_h, dkg_h))]
        )
    ]
    for c in loads:
        c.start()
    quarter = length // 4
    token_loads = [
        pltpu.make_async_copy(
            tokens.at[pl.ds(i * quarter, quarter)], x.at[pl.ds(i * quarter, quarter)], load_sems[8 + i]
        )
        for i in range(4)
    ]
    for c in token_loads + small:
        c.start()
    for c in loads[:4]:
        c.wait()
    for at, base in ((0, 128), (2, 384)):
        pair = jnp.concatenate([stage[at], stage[at + 1]], axis=0).astype(F32)
        wall[me, :, base : base + 128] = pair.T.astype(BF16)
    for c in loads[4:]:
        c.wait()
    pl.semaphore_wait(barrier, 6)

    pair_rows = (kp.shape[1] // 2, vt.shape[1] // 2)
    in_ring = PairRing(me, n_sp, wall, depth * 5 // 16, side, other, in_s, in_r, in_ys, in_yr)
    out_ring = PairRing(me, n_sp, oall, 128, side, other, out_s, out_r, out_ys, out_yr)
    kv_ring = Ring(
        me, n_sp, 4,
        lambda w, p: (kp, vt)[p // 2].at[w, pl.ds(p % 2 * (pair_rows[p // 2]), pair_rows[p // 2])],
        kv_snd, in_r,
    )
    in_ring.begin()
    for c in small:
        c.wait()

    def norm(i):
        token_loads[i].wait()

        def norm_rows(r, carry):
            at = pl.multiple_of(i * quarter + r * 16, 16)
            total = jnp.zeros((16, 128), F32)
            for j in range(width // 128):
                piece = x[pl.ds(at, 16), j * 128 : j * 128 + 128].astype(F32)
                total = total + piece * piece
            scale = lax.rsqrt(jnp.sum(total, axis=-1, keepdims=True) * (1.0 / width) + EPS)
            for j in range(width // 128):
                piece = x[pl.ds(at, 16), j * 128 : j * 128 + 128].astype(F32)
                x[pl.ds(at, 16), j * 128 : j * 128 + 128] = (
                    piece * scale * gain[j : j + 1, :]
                ).astype(BF16)
            return carry

        lax.fori_loop(0, quarter // 16, norm_rows, 0)

    lane = lax.broadcasted_iota(jnp.int32, (1, 128), 1)
    low_lane = lane < HD

    def tables(r, carry):
        at = pl.multiple_of(r * 64, 64)
        place = me * length + at + lax.broadcasted_iota(jnp.int32, (64, 128), 0)
        angle = place.astype(F32) * freq[0:1, :]
        table[0, pl.ds(at, 64)] = jnp.cos(angle)
        table[1, pl.ds(at, 64)] = jnp.sin(angle)
        row = lax.div(place, GRID_W)
        spot = jnp.where(lax.rem(lane, HD) < HD // 2, row, place - row * GRID_W)
        angle = spot.astype(F32) * freq[1:2, :]
        table[2, pl.ds(at, 64)] = jnp.cos(angle)
        table[3, pl.ds(at, 64)] = jnp.sin(angle)
        return carry

    def project(w, first=False):
        at = pl.multiple_of(w * depth, depth)
        product = nn(x[:, pl.ds(at, depth)], wall[w])
        if first:
            acc[...] = product
        else:
            acc[...] += product

    def projects(d, carry):
        in_ring.take(d)
        project(in_ring.owner(0, d))
        project(in_ring.owner(1, d))
        return carry

    def in_step(d, carry):
        in_ring.hop_piece(d, 0)
        in_ring.hop_piece(d, 1)

        @pl.when(d == 1)
        def _():
            norm(0)
            norm(1)

        @pl.when(d == 2)
        def _():
            norm(2)
            norm(3)

        @pl.when(d == 3)
        def _():
            lax.fori_loop(0, length // 64, tables, 0)
            project(me, first=True)

        @pl.when(d >= 4)
        def _():
            lax.fori_loop(jnp.where(d == 4, 1, d - 2), d - 1, projects, 0)

        in_ring.hop_piece(d, 2)
        in_ring.hop_piece(d, 3)
        return carry

    lax.fori_loop(1, half, in_step, 0)
    out_ring.begin()
    projects(half - 2, 0)
    in_ring.last_first()
    projects(half - 1, 0)
    in_ring.last_second()
    for p in range(2):
        out_ring.hop_piece(1, p)
    in_ring.take_last()
    project(in_ring.owner(0, half))

    def two(which):
        return jnp.concatenate([gains[which], gains[which]], axis=1)

    def heads(values, g, which, reach, rows):
        squares = values * values
        low = jnp.sum(jnp.where(low_lane, squares, 0.0), axis=-1, keepdims=True)
        high = jnp.sum(jnp.where(low_lane, 0.0, squares), axis=-1, keepdims=True)
        mean = jnp.where(low_lane, low, high) * (1.0 / HD)
        normed = values * lax.rsqrt(mean + EPS) * g
        turned = jnp.where(
            lax.rem(lane, 2 * reach) < reach,
            -pltpu.roll(normed, 128 - reach, 1),
            pltpu.roll(normed, reach, 1),
        )
        return normed * table[which, rows] + turned * table[which + 1, rows]

    blocks = [slice(i * 128, i * 128 + 128) for i in range(length // 128)]
    g = two(3)
    keys = [
        heads(acc[rows, 384:512], g, 2, HD // 4, rows)
        for rows in (slice(0, half_rows), slice(half_rows, length))
    ]
    kp[me] = jnp.where(low_lane, keys[0], pltpu.roll(keys[1], HD, 1)).astype(BF16)
    for rows in blocks:
        vt[me, :, rows] = acc[rows, 384:512].T[HD:].astype(BF16)
    kv_ring.begin((0, 1))
    g = two(1)
    for i, rows in enumerate(blocks):
        values = acc[rows, 128:256]
        kvw[pl.ds(WINDOW + i * 128, 128)] = jnp.where(
            low_lane, heads(values, g, 0, HD // 2, rows), values
        ).astype(BF16)
    kv_ring.begin((2, 3))
    halos = [
        remote(
            kvw.at[pl.ds(length, WINDOW)], kvw.at[pl.ds(0, WINDOW)], halo_s.at[0], halo_r.at[0], right
        ),
        remote(
            kvw.at[pl.ds(WINDOW, WINDOW)],
            kvw.at[pl.ds(WINDOW + length, WINDOW)],
            halo_s.at[1],
            halo_r.at[1],
            left,
        ),
    ]
    for c in halos:
        c.start()
    scale = HD ** (-0.5)
    g = two(2)
    for rows in blocks:
        q = heads(acc[rows, 256:384], g, 2, HD // 4, rows) * (scale * math.log2(math.e))
        q = q.T.astype(BF16)
        for h in range(2):
            for p in range(2):
                cols_h = slice(h * length + rows.start, h * length + rows.stop)
                qd[p, p * HD : p * HD + HD, cols_h] = q[h * HD : h * HD + HD]
                qd[p, (1 - p) * HD : (1 - p) * HD + HD, cols_h] = jnp.zeros((HD, 128), BF16)
    g = two(0)
    for rows in blocks:
        q = heads(acc[rows, 0:128], g, 0, HD // 2, rows).astype(BF16).astype(F32) * scale
        qw[0, rows] = jnp.where(low_lane, q, 0.0).astype(BF16)
        qw[1, rows] = jnp.where(low_lane, pltpu.roll(q, HD, 1), 0.0).astype(BF16)

    m_s[...] = jnp.full(m_s.shape, LOW, F32)
    a_s[...] = jnp.zeros(a_s.shape, F32)

    def window(i):
        at = pl.multiple_of(i * 128, 128)
        queries = jnp.concatenate([qw[0, pl.ds(at, 128)], qw[1, pl.ds(at, 128)]], axis=0)
        near = kvw[pl.ds(at, 3 * WINDOW)]
        scores = nt(queries, near)
        row = lax.broadcasted_iota(jnp.int32, scores.shape, 0)
        key = lax.broadcasted_iota(jnp.int32, scores.shape, 1)
        first = row < 128
        spot = jnp.where(first, row, row - 128)
        place = me * length + at - WINDOW + key
        valid = (
            (key >= spot)
            & (key <= spot + 2 * WINDOW)
            & (place >= 0)
            & (place < length * n_sp)
        )
        scores = jnp.where(valid, scores, LOW)
        floor = jnp.where(
            lax.broadcasted_iota(jnp.int32, (256, 1), 0) < 128, sink[0], sink[1]
        )
        top = jnp.maximum(jnp.max(scores, axis=-1, keepdims=True), floor)
        expon = jnp.exp(scores - top)
        total = jnp.sum(expon, axis=-1, keepdims=True) + jnp.exp(floor - top)
        weights = (expon / total).astype(BF16)
        result = nn(weights, near)
        attw[0, pl.ds(at, 128)] = jnp.where(
            low_lane, pltpu.roll(result[:128], HD, 1), result[128:]
        ).astype(BF16)

    ones = jnp.ones((8, 2 * length), BF16)

    def dense(owners, cut=slice(None)):
        keys = jnp.concatenate([kp[w] for w in owners], axis=0)
        values = jnp.concatenate(
            [jnp.concatenate([vt[w] for w in owners], axis=1), ones], axis=0
        )
        low, high = nn(keys, qd[0, :, cut]), nn(keys, qd[1, :, cut])
        before = m_s[:, cut]
        top = jnp.maximum(before, jnp.max(jnp.maximum(low, high), axis=0, keepdims=True))
        shrink = jnp.exp2(before - top)
        low = jnp.exp2(low - top[:1]).astype(BF16)
        high = jnp.exp2(high - top[:1]).astype(BF16)
        expons = jnp.concatenate(
            [low[:half_rows], high[:half_rows], low[half_rows:], high[half_rows:]], axis=0
        )
        a_s[:, cut] = a_s[:, cut] * shrink[:1] + nn(values, expons)
        m_s[:, cut] = top

    def kv_step(d, carry):
        for h in range(2):

            @pl.when(d < half)
            def _():
                kv_ring.hop_piece(d, 2 * h)
                kv_ring.hop_piece(d, 2 * h + 1)

            @pl.when(d >= 2)
            def _():
                dense(
                    (kv_ring.owner(0, d - 1), kv_ring.owner(1, d - 1)),
                    slice(h * length, h * length + length),
                )

        @pl.when(d + EARLY < half)
        def _():
            out_ring.hop_piece(d + EARLY, 0)

        @pl.when((d >= 3) & (d < 3 + length // 128))
        def _():
            window(d - 3)

        @pl.when(d + EARLY < half)
        def _():
            out_ring.hop_piece(d + EARLY, 1)

        @pl.when(d + EARLY == half)
        def _():
            out_ring.last()

        @pl.when(d == 2)
        def _():
            for c in halos:
                c.wait_recv()

        return carry

    for h in range(2, EARLY + 1):
        for p in range(2):
            out_ring.hop_piece(h, p)
    lax.fori_loop(1, half + 1, kv_step, 0)
    kv_ring.last()
    dense((me, kv_ring.owner(0, half)))
    both = jnp.concatenate(
        [a_s[:HD, h * length : h * length + length] / a_s[HD : HD + 1, h * length : h * length + length] for h in range(2)],
        axis=0,
    )
    for rows in blocks:
        attw[1, rows] = both[:, rows].T.astype(BF16)
    for t in range(n_tp):
        at = (t % 2) * half_rows + (t // 2) * share
        for which in range(2):
            att[at : at + share, which * 128 : which * 128 + 128] = attw[
                which, t * share : t * share + share
            ]

    def owners_of(s):
        return (
            lax.rem(me + n_sp - lax.rem(s, half), n_sp),
            lax.rem(me + s, n_sp),
        )

    theirs_at = pl.multiple_of((1 - core) * half_rows, half_rows)
    mine_at = pl.multiple_of(core * half_rows, half_rows)
    up = lax.rem(xc + 1, n_x)
    down = lax.rem(xc + n_x - 1, n_x)
    far = lax.rem(xc + 2, n_x)
    ways = ((x_up, up, x_down, down), (x_down, down, x_up, up))

    def pair_copy(s):
        return remote(dsend.at[s], drecv.at[s], d_s.at[lax.rem(s, 2)], d_r.at[s], partner)

    def far_copy(s, b):
        return remote(xs.at[s, b, far], r2.at[s, b], in_s.at[0, b, lax.rem(s, 4)], x_r.at[0, s, b], ways[b][0])

    def chain_copy(s, b):
        return remote(c1.at[s, b], rc.at[s, b], in_s.at[1, b, lax.rem(s, 4)], x_r.at[1, s, b], ways[b][0])

    def near_copy(s, b):
        return remote(
            xs.at[s, b, ways[b][3]], rd.at[s, b], out_s.at[b, lax.div(lax.rem(s, 4), 2), lax.rem(s, 2)], x_r.at[2, s, b], ways[b][2]
        )

    def stage1(s):
        owners = owners_of(s)
        for b in range(2):
            dsend[s - 1, b] = nn(att[pl.ds(theirs_at, half_rows)], oall[owners[b]]).astype(BF16)
        mine[s - 1, 0] = nn(att[pl.ds(mine_at, half_rows)], oall[owners[0]])

        @pl.when(s > 2)
        def _():
            pair_copy(s - 3).wait_send()

        pair_copy(s - 1).start()
        mine[s - 1, 1] = nn(att[pl.ds(mine_at, half_rows)], oall[owners[1]])

    def stage2(s):
        pair_copy(s - 1).wait_recv()
        for b in range(2):
            both = (mine[s - 1, b] + drecv[s - 1, b].astype(F32)).astype(BF16)
            for t in range(n_x):
                xs[s - 1, b, t] = both[t * share : t * share + share]

        @pl.when(s > 4)
        def _():
            for b in range(2):
                far_copy(s - 5, b).wait_send()

        for b in range(2):
            far_copy(s - 1, b).start()

    def stage3(s):
        for b in range(2):
            far_copy(s - 1, b).wait_recv()
            c1[s - 1, b] = (xs[s - 1, b, ways[b][1]].astype(F32) + r2[s - 1, b].astype(F32)).astype(
                BF16
            )

        @pl.when(s > 4)
        def _():
            for b in range(2):
                chain_copy(s - 5, b).wait_send()

        for b in range(2):
            chain_copy(s - 1, b).start()

    def send_near(s):
        @pl.when(s > 4)
        def _():
            for b in range(2):
                near_copy(s - 5, b).wait_send()

        for b in range(2):
            near_copy(s - 1, b).start()

    def stage4(s):
        for b in range(2):
            chain_copy(s - 1, b).wait_recv()
            near_copy(s - 1, b).wait_recv()
            total = (
                xs[s - 1, b, xc].astype(F32) + rc[s - 1, b].astype(F32) + rd[s - 1, b].astype(F32)
            )
            at = pl.multiple_of(owners_of(s)[b] * cols, cols)
            out[:, pl.ds(at, cols)] = total.astype(BF16)

    def out_step(s, carry):
        @pl.when(s < half)
        def _():
            out_ring.take(s)

        @pl.when(s == half)
        def _():
            out_ring.take_last()

        @pl.when(s <= half)
        def _():
            stage1(s)

        @pl.when((s >= 1 + LAG[0]) & (s <= half + LAG[0]))
        def _():
            stage2(s - LAG[0])

        @pl.when((s >= 1 + LAG[1]) & (s <= half + LAG[1]))
        def _():
            stage3(s - LAG[1])

        @pl.when((s >= 1 + LAG[2]) & (s <= half + LAG[2]))
        def _():
            send_near(s - LAG[2])

        @pl.when(s >= 1 + LAG[3])
        def _():
            stage4(s - LAG[3])

        @pl.when(s == 3)
        def _():
            in_ring.drain_pair()
            kv_ring.drain()
            for c in halos:
                c.wait_send()

        return carry

    in_ring.drain()
    out_ring.drain()
    lax.fori_loop(1, half + LAG[3] + 1, out_step, 0)

    out_ring.drain_pair()

    def drain(s, carry):
        for b in range(2):
            far_copy(s, b).wait_send()
            near_copy(s, b).wait_send()
            chain_copy(s, b).wait_send()
        return carry

    lax.fori_loop(half - 4, half, drain, 0)
    for s in (half - 2, half - 1):
        pair_copy(s).wait_send()


def frequencies():
    lane = np.arange(128)
    line = THETA ** (-2.0 * (lane % (HD // 2)) / HD)
    grid = THETA ** (-2.0 * (lane % (HD // 4)) / (HD // 2))
    return np.stack([line, grid]).astype(np.float32)


def solution(mesh):
    n_sp, n_tp = mesh.shape["sp"], mesh.shape["tp"]
    assert n_sp % 2 == 0 and n_tp == 8 and mesh.shape["grp"] % 2 == 0

    def local(tokens, gain, wq, wk, wv, wqg, wkg, sink, dq, dk, dv, dqg, dkg, wo, do):
        length, width = tokens.shape
        depth, cols = wq.shape[0], wo.shape[1]
        half, n_x, share = n_sp // 2, n_tp // 2, length // n_tp
        assert wq.shape[1] == dq.shape[1] == 2 * HD and wk.shape[1] == dk.shape[1] == HD
        assert length % 128 == 0 and share % 16 == 0 and width == depth * n_sp
        any_ = pl.BlockSpec(memory_space=pl.ANY)
        smem = pl.BlockSpec(memory_space=pltpu.SMEM)
        dma = pltpu.SemaphoreType.DMA
        return pl.pallas_call(
            functools.partial(kernel, n_sp, n_tp),
            out_shape=pltpu.VMEM((share, cols * n_sp), BF16),
            in_specs=[any_] * 7 + [smem] + [any_] * 8,
            out_specs=pl.BlockSpec(memory_space=pltpu.VMEM),
            scratch_shapes=[
                pltpu.VMEM((length, width), BF16),
                pltpu.VMEM((n_sp, depth, 512), BF16),
                pltpu.VMEM((4, HD, depth), BF16),
                pltpu.VMEM((length, 512), F32),
                pltpu.VMEM((n_sp, 256, cols), BF16),
                pltpu.VMEM((n_sp, length // 2, 128), BF16),
                pltpu.VMEM((n_sp, HD, length), BF16),
                pltpu.VMEM((length + 2 * WINDOW, 128), BF16),
                pltpu.VMEM((2, 128, 2 * length), BF16),
                pltpu.VMEM((2, length, 128), BF16),
                pltpu.VMEM((length, 256), BF16),
                pltpu.VMEM((2, length, 128), BF16),
                pltpu.VMEM((8, 2 * length), F32),
                pltpu.VMEM((HD + 8, 2 * length), F32),
                pltpu.VMEM((4, length, 128), F32),
                pltpu.VMEM((half, 2, length // 2, cols), BF16),
                pltpu.VMEM((half, 2, length // 2, cols), BF16),
                pltpu.VMEM((half, 2, length // 2, cols), F32),
                pltpu.VMEM((half, 2, n_x, share, cols), BF16),
                pltpu.VMEM((half, 2, share, cols), BF16),
                pltpu.VMEM((half, 2, share, cols), BF16),
                pltpu.VMEM((half, 2, share, cols), BF16),
                pltpu.VMEM((half, 2, share, cols), BF16),
                dma((2, 2, 4)),
                dma((2, half, 4)),
                dma((2, 2, 2)),
                dma((2, half, 2)),
                dma((2,)),
                dma((2,)),
                dma((2,)),
                dma((half,)),
                dma((3, half, 2)),
                dma((2, 2)),
                dma((2, half)),
                dma((2, 2)),
                dma((2, half)),
                pltpu.VMEM((width // 128, 128), F32),
                pltpu.VMEM((4, 1, HD), F32),
                pltpu.VMEM((2, 128), F32),
                dma((2, 2, 4)),
            ],
            compiler_params=pltpu.CompilerParams(
                collective_id=0, has_side_effects=True, vmem_limit_bytes=60 * 1024 * 1024
            ),
        )(
            tokens, gain.reshape(-1, 128), wq, wk.T, wv.T, wqg[None], wkg[None], sink,
            dq, dk.T, dv.T, dqg[None], dkg[None], wo, do, jnp.asarray(frequencies()),
        )

    return jax.shard_map(
        local,
        mesh=mesh,
        in_specs=(
            P(("grp", "sp"), None),
            P(),
            P("sp", "tp"),
            P("sp", "tp"),
            P("sp", "tp"),
            P(),
            P(),
            P("tp"),
            P("sp", "tp"),
            P("sp", "tp"),
            P("sp", "tp"),
            P(),
            P(),
            P("tp", "sp"),
            P("tp", "sp"),
        ),
        out_specs=P(("grp", "sp", "tp"), None),
        check_vma=False,
    )
```
